32 devices in a mesh: dp: 2 (over x), kv: 8 (over z, y), tp: 2 (over core).
Axes of the slice: x: 2, y: 2, z: 4, core: 2. Of those that a mesh axis runs over, the one named last changes fastest.
Arguments:
- tokens: bfloat16 [4096, 2048], P(('dp', 'kv')), parts along dimension 0, may hold values from -6 to 6
- query_weight: bfloat16 [2048, 1024], P(None, 'tp'), as said below
- key_weight: bfloat16 [2048, 128], replicated, as said below
- value_weight: bfloat16 [2048, 128], replicated, may hold values from -0.125 to 0.125
- gate_weight: bfloat16 [2048, 32], replicated, may hold values from -0.125 to 0.125
- key_inner: bfloat16 [2048, 64], replicated, as said below
- key_outer: bfloat16 [64, 64], replicated, as said below
- value_inner: bfloat16 [2048, 64], replicated, may hold values from -0.125 to 0.125
- value_outer: bfloat16 [64, 64], replicated, may hold values from -0.75 to 0.75
- out_weight: bfloat16 [1024, 2048], P(None, 'tp'), may hold values from -0.75 to 0.75
- selection: int32 [2, 64, 8], P('tp', ('dp', 'kv')), parts along dimension 1, may hold values from -1 to 31, as said below
Outputs:
- mixed_out: bfloat16 [4096, 2048], P(('dp', 'kv'), 'tp'), parts along dimension 0
The draws below stay inside these ranges and needn't reach their ends.
There are 2 independent parts, one for each index of `dp`. The reference program is written for one: setup_inputs(seed, part) draws one part's arguments, and reference() takes and returns one part's arrays. A program takes and returns all parts, laid end to end along the dimension named above; an argument that names none is the same for every part. Nothing has to cross between parts.
Inputs may be any that keep to these rules, and one draw needn't show every extreme that they name: Slot 0 of selection[g, b] is block b itself; the other slots name distinct blocks before b, or -1 where fewer than 7 blocks lie before b. `query_weight`: every entry lies within six over the square root of 2048 of zero. `key_weight`: every entry lies within six over the square root of 2048 of zero. `key_inner`: every entry lies within six over the square root of 2048 of zero. `key_outer`: every entry lies within six over the square root of 64 of zero.
All inputs are finite; a program needn't handle non-finite values.
Results may differ from the reference program's by a relative error of at most 0.0093.
Values may be sent and summed in bfloat16 or wider, within the bound.
A program may use at most 64 MiB of HBM per device.

```python
import jax
import jax.numpy as jnp
from jax import lax

WIDTH = 2048
HEADS = 16
HEAD_DIM = 64
KV_HEADS = 2
BLOCK = 64
SPAN = 32
PICKS = 8
TOK_DEV = 256
LENGTH = 2048
N_KV = 8


def bounded(values, fan_in):
    bound_value = 6.0 * fan_in ** (-0.5)
    return jnp.clip(values, -bound_value, bound_value).astype(jnp.bfloat16)


def draw_query_weight(key, part):
    values = jax.random.normal(jax.random.fold_in(key, 101), (WIDTH, HEADS * HEAD_DIM), jnp.float32) * WIDTH ** (-0.5)
    return bounded(values, WIDTH)


def draw_key_weight(key, part):
    values = jax.random.normal(jax.random.fold_in(key, 102), (WIDTH, KV_HEADS * HEAD_DIM), jnp.float32) * WIDTH ** (-0.5)
    return bounded(values, WIDTH)


def draw_key_inner(key, part):
    fan_value = SPAN * HEAD_DIM
    values = jax.random.normal(jax.random.fold_in(key, 103), (fan_value, HEAD_DIM), jnp.float32) * fan_value ** (-0.5)
    return bounded(values, fan_value)


def draw_key_outer(key, part):
    values = jax.random.normal(jax.random.fold_in(key, 104), (HEAD_DIM, HEAD_DIM), jnp.float32) * HEAD_DIM ** (-0.5)
    return bounded(values, HEAD_DIM)


def draw_tokens(key, part):
    normal_rows = jax.random.normal(jax.random.fold_in(key, 201), (LENGTH, WIDTH), jnp.float32)
    normal_rows = jnp.clip(normal_rows, -6.0, 6.0)
    return normal_rows.astype(jnp.bfloat16)


def draw_selection(key, part):
    block_count = TOK_DEV * N_KV // BLOCK
    per_device = TOK_DEV // BLOCK
    hot_key, noise_key = jax.random.split(key)
    hotness = jax.random.randint(hot_key, (KV_HEADS, 1, block_count), 0, 4)
    noise = jax.random.randint(noise_key, (KV_HEADS, block_count, block_count), 0, 65536)
    query_ids = jnp.arange(block_count).astype(jnp.int32)[:, None]
    key_ids = jnp.arange(block_count).astype(jnp.int32)[None, :]
    forced = (key_ids == query_ids - per_device) | (key_ids == query_ids - block_count // 2)
    priority = jnp.where(forced[None], 262144, noise + hotness * 32768)
    ranked = jnp.where((key_ids < query_ids)[None], priority * 2048 + key_ids[None], -1 - key_ids[None])
    ranked_values, picked_ids = lax.top_k(ranked, PICKS - 1)
    earlier = jnp.where(ranked_values >= 0, picked_ids, -1).astype(jnp.int32)
    own_block = jnp.broadcast_to(query_ids[None], (KV_HEADS, block_count, 1)).astype(jnp.int32)
    return jnp.concatenate([own_block, earlier], axis=2)


def block_levels(own_key, extent, cuts, low, largest):
    gain, own = 1.0, jax.random.fold_in(own_key, 6)
    for axis_at, parts in cuts:
        draws = jnp.exp(jax.random.uniform(jax.random.fold_in(own, axis_at), (parts,), jnp.float32, low / len(cuts), largest / len(cuts)))
        gain = gain * jnp.repeat(draws, extent[axis_at] // parts).reshape([-1 if axis == axis_at else 1 for axis in range(len(extent))])
    return gain


def bell_draw(own_key, dims, scale, most, cuts=(), dtype=jnp.bfloat16):
    loudness = block_levels(own_key, dims, cuts, -0.22, 0.18) if cuts else 1.0
    array = jax.random.normal(own_key, dims, jnp.float32) * scale * loudness
    return jnp.minimum(jnp.maximum(array, -most), most).astype(dtype)


def setup_inputs(seed: int = 0, part: int = 0) -> dict:
    arg_keys = jax.random.split(jax.random.key(seed), 12)
    part_keys = jax.random.split(jax.random.fold_in(arg_keys[11], part), 12)
    return {
        "tokens": draw_tokens(jax.random.fold_in(jax.random.fold_in(arg_keys[11], part), 71), part),
        "query_weight": draw_query_weight(jax.random.fold_in(arg_keys[11], 71), part),
        "key_weight": draw_key_weight(jax.random.fold_in(arg_keys[11], 71), part),
        "value_weight": bell_draw(arg_keys[3], (WIDTH, KV_HEADS * HEAD_DIM), WIDTH ** -0.5, 0.125),
        "gate_weight": bell_draw(arg_keys[4], (WIDTH, 2 * HEADS), WIDTH ** -0.5, 0.125),
        "key_inner": draw_key_inner(jax.random.fold_in(arg_keys[11], 71), part),
        "key_outer": draw_key_outer(jax.random.fold_in(arg_keys[11], 71), part),
        "value_inner": bell_draw(arg_keys[7], (SPAN * HEAD_DIM, HEAD_DIM), (SPAN * HEAD_DIM) ** -0.5, 0.125),
        "value_outer": bell_draw(arg_keys[8], (HEAD_DIM, HEAD_DIM), HEAD_DIM ** -0.5, 0.75),
        "out_weight": bell_draw(arg_keys[9], (HEADS * HEAD_DIM, WIDTH), HEAD_DIM ** -0.5, 0.75, ((1, 2),)),
        "selection": draw_selection(jax.random.fold_in(jax.random.fold_in(arg_keys[11], part), 71), part),
    }


def masked_softmax(scores, allowed, over_axes):
    shifted = jnp.where(allowed, scores, -1e30)
    row_max = jnp.max(shifted, axis=over_axes, keepdims=True)
    weights = jnp.where(allowed, jnp.exp(shifted - row_max), 0.0)
    row_total = jnp.sum(weights, axis=over_axes, keepdims=True)
    return (weights / jnp.maximum(row_total, 1.0)).astype(jnp.bfloat16)


def summarize(key_block, inner_weight, outer_weight):
    flattened = key_block.reshape(-1, SPAN * HEAD_DIM)
    hidden = jax.nn.gelu(jnp.dot(flattened, inner_weight, preferred_element_type=jnp.float32)).astype(jnp.bfloat16)
    return jnp.dot(hidden, outer_weight, preferred_element_type=jnp.float32).astype(jnp.bfloat16)


def reference(tokens, query_weight, key_weight, value_weight, gate_weight, key_inner, key_outer, value_inner, value_outer, out_weight, selection):
    length = tokens.shape[0]
    per_group = HEADS // KV_HEADS
    queries = jnp.dot(tokens, query_weight, preferred_element_type=jnp.float32).astype(jnp.bfloat16)
    queries = queries.reshape(length, KV_HEADS, per_group, HEAD_DIM)
    key_rows = jnp.dot(tokens, key_weight, preferred_element_type=jnp.float32).astype(jnp.bfloat16).reshape(length, KV_HEADS, HEAD_DIM)
    value_rows = jnp.dot(tokens, value_weight, preferred_element_type=jnp.float32).astype(jnp.bfloat16).reshape(length, KV_HEADS, HEAD_DIM)
    gate_values = jax.nn.sigmoid(jnp.dot(tokens, gate_weight, preferred_element_type=jnp.float32))
    summary_keys = jnp.stack([summarize(key_rows[:, group], key_inner, key_outer) for group in range(KV_HEADS)], axis=1)
    summary_values = jnp.stack([summarize(value_rows[:, group], value_inner, value_outer) for group in range(KV_HEADS)], axis=1)
    summary_count = length // SPAN
    block_count = length // BLOCK
    score_scale = HEAD_DIM ** -0.5
    summary_ends = (jnp.arange(summary_count) * SPAN + SPAN - 1).astype(jnp.int32)
    offsets = jnp.arange(BLOCK).astype(jnp.int32)
    summary_kf = summary_keys.astype(jnp.float32)
    summary_vf = summary_values.astype(jnp.float32)

    def take_rows(source_rows, row_ids):
        return source_rows[row_ids]

    def one_block(block_index):
        first_row = block_index * BLOCK
        query_block = lax.dynamic_slice_in_dim(queries, first_row, BLOCK, 0).astype(jnp.float32)
        places = first_row + offsets
        scores = jnp.einsum('qghd,ngd->ghqn', query_block, summary_kf) * score_scale
        allowed = summary_ends[None, :] <= places[:, None]
        summary_weights = masked_softmax(scores, allowed[None, None], (3,))
        summary_out = jnp.einsum('ghqn,ngd->qghd', summary_weights.astype(jnp.float32), summary_vf)
        picked = lax.dynamic_index_in_dim(selection, block_index, 1, keepdims=False)
        positions = picked[:, :, None] * BLOCK + offsets
        row_index = jnp.clip(positions, 0, length - 1).astype(jnp.int32)
        picked_keys = jax.vmap(take_rows, in_axes=(1, 0))(key_rows, row_index).astype(jnp.float32)
        picked_values = jax.vmap(take_rows, in_axes=(1, 0))(value_rows, row_index).astype(jnp.float32)
        chosen_scores = jnp.einsum('qghd,gpld->ghqpl', query_block, picked_keys) * score_scale
        chosen_allowed = (picked >= 0)[:, None, :, None] & (positions[:, None, :, :] <= places[None, :, None, None])
        chosen_weights = masked_softmax(chosen_scores, chosen_allowed[:, None], (3, 4))
        chosen_out = jnp.einsum('ghqpl,gpld->qghd', chosen_weights.astype(jnp.float32), picked_values)
        gate_block = lax.dynamic_slice_in_dim(gate_values, first_row, BLOCK, 0)
        summary_gate = gate_block[:, :HEADS].reshape(BLOCK, KV_HEADS, per_group, 1)
        chosen_gate = gate_block[:, HEADS:].reshape(BLOCK, KV_HEADS, per_group, 1)
        mixed = (summary_gate * summary_out + chosen_gate * chosen_out).astype(jnp.bfloat16)
        return mixed.reshape(BLOCK, HEADS * HEAD_DIM)

    mixed = lax.map(one_block, jnp.arange(block_count).astype(jnp.int32)).reshape(length, HEADS * HEAD_DIM)
    return jnp.dot(mixed, out_weight, preferred_element_type=jnp.float32).astype(jnp.bfloat16)
```

```python
import functools

import jax
import jax.numpy as jnp
from jax import lax
from jax.experimental import pallas as pl
from jax.experimental.pallas import tpu as pltpu
from jax.sharding import PartitionSpec as P

HEAD_DIM = 64
BLOCK = 64
SPAN = 32
LANES = 128
MESH = pl.DeviceIdType.MESH
F32 = jnp.float32
BF16 = jnp.bfloat16
CHUNKS = 4
PARTS = 2
LOG2E = 1.4426950408889634
GRANT = 40 * 1024 * 1024


def dot(a, b):
    return jnp.dot(a, b, preferred_element_type=F32)


def dot_t(a, b):
    return lax.dot_general(a, b, (((1,), (1,)), ((), ())), preferred_element_type=F32)


def dot_rows(a, b):
    return lax.dot_general(a, b, (((0,), (0,)), ((), ())), preferred_element_type=F32)


def low_half(shape):
    return lax.broadcasted_iota(jnp.int32, shape, len(shape) - 1) < HEAD_DIM


def kernel(
    n_kv,
    inner,
    sel_hbm,
    tok_hbm,
    qw_hbm,
    kw_hbm,
    vw_hbm,
    gw_hbm,
    kin_hbm,
    kout_hbm,
    vin_hbm,
    vout_hbm,
    ow_hbm,
    out_ref,
    sel,
    tok,
    qw,
    kvw,
    gw,
    kin,
    kout,
    vin,
    vout,
    ow,
    rows32,
    gathered,
    sums,
    stacked,
    summary_mix,
    gate_rows,
    own_mix,
    peer_mix,
    partial,
    load_sem,
    ready,
    send_z,
    recv_z,
    send_y,
    recv_y,
    send_s,
    recv_s,
    send_m,
    recv_m,
):
    local, width = tok.shape
    runs = local // SPAN
    blocks = local // BLOCK
    cols = qw.shape[1]
    heads = cols // HEAD_DIM
    pairs = cols // LANES
    picks = sel.shape[2]
    outer = n_kv // inner
    me = lax.axis_index("kv")
    g = lax.axis_index("tp")
    z = me // inner
    y = lax.rem(me, inner)

    barrier = pltpu.get_barrier_semaphore()

    def greet(target, carry):
        pl.semaphore_signal(barrier, inc=1, device_id={"kv": target}, device_id_type=MESH)
        return carry

    lax.fori_loop(me + 1, n_kv, greet, 0)
    pl.semaphore_signal(barrier, inc=1, device_id={"tp": 1 - g}, device_id_type=MESH)

    depth = width // CHUNKS
    first = []
    for c in range(CHUNKS):
        part = pl.ds(c * depth, depth)
        trio = [
            pltpu.make_async_copy(tok_hbm.at[:, part], tok.at[:, part], load_sem.at[3 * c]),
            pltpu.make_async_copy(
                kw_hbm.at[part], kvw.at[part, pl.ds(0, LANES)], load_sem.at[3 * c + 1]
            ),
            pltpu.make_async_copy(
                vw_hbm.at[part], kvw.at[part, pl.ds(LANES, LANES)], load_sem.at[3 * c + 2]
            ),
        ]
        for copy in trio:
            copy.start()
        first.append(trio)
    base = 3 * CHUNKS
    later = [
        pltpu.make_async_copy(src, dst, load_sem.at[base + i])
        for i, (src, dst) in enumerate(
            [
                (kin_hbm, kin),
                (vin_hbm, vin),
                (kout_hbm, kout),
                (vout_hbm, vout),
                (qw_hbm, qw),
                (gw_hbm, gw),
                (sel_hbm, sel),
                (ow_hbm, ow),
            ]
        )
    ]
    kin_c, vin_c, kout_c, vout_c, qw_c, gw_c, sel_c, ow_c = later

    sums[...] = jnp.zeros_like(sums)
    pl.semaphore_wait(barrier, me + 1)

    def tell(target, carry):
        pl.semaphore_signal(ready.at[me], inc=1, device_id={"kv": target}, device_id_type=MESH)
        return carry

    lax.fori_loop(0, me, tell, 0)

    acc = jnp.zeros((local, 2 * LANES), F32)
    for c in range(CHUNKS):
        for copy in first[c]:
            copy.wait()
        if c == CHUNKS - 2:
            for copy in later:
                copy.start()
        part = pl.ds(c * depth, depth)
        acc += dot(tok[:, part], kvw[part, :])
    keys = acc[:, :LANES]
    values = acc[:, LANES:]
    low = low_half((local, LANES))
    paired = jnp.where(
        g == 0,
        jnp.where(low, keys, pltpu.roll(values, HEAD_DIM, 1)),
        jnp.where(low, pltpu.roll(keys, HEAD_DIM, 1), values),
    ).astype(BF16)
    gathered[pl.ds(me * blocks, blocks)] = paired.reshape(blocks, BLOCK, LANES)
    rows32[...] = paired.astype(F32)

    part_blocks = blocks // PARTS

    def slot(index, part):
        return gathered.at[pl.ds(index * blocks + part * part_blocks, part_blocks)]

    def z_copy(source_z, target_z, part):
        return pltpu.make_async_remote_copy(
            src_ref=slot(source_z * inner + y, part),
            dst_ref=slot(source_z * inner + y, part),
            send_sem=send_z.at[target_z, part],
            recv_sem=recv_z.at[source_z, part],
            device_id={"kv": target_z * inner + y},
            device_id_type=MESH,
        )

    def y_copy(source_z, source_y, part):
        return pltpu.make_async_remote_copy(
            src_ref=slot(source_z * inner + source_y, part),
            dst_ref=slot(source_z * inner + source_y, part),
            send_sem=send_y.at[source_z, part],
            recv_sem=recv_y.at[source_z, part],
            device_id={"kv": z * inner + lax.rem(y + 1, inner)},
            device_id_type=MESH,
        )

    def wait_ready(index):
        pl.semaphore_wait(ready.at[index], 1)

    def z_send(target, carry):
        wait_ready(target * inner + y)
        for part in range(PARTS):
            z_copy(z, target, part).start()
        return carry

    lax.fori_loop(z + 1, jnp.minimum(z + 2, outer), z_send, 0)
    if inner == 2:

        @pl.when(y == 0)
        def _():
            wait_ready(me + 1)
            for part in range(PARTS):
                y_copy(z, 0, part).start()

    steps = [rows32[pl.ds(j, runs, stride=SPAN), :] for j in range(SPAN)]
    low8 = low_half((runs, LANES))
    flat_k = jnp.concatenate(
        [
            jnp.where(low8, steps[j], pltpu.roll(steps[j + 1], HEAD_DIM, 1))
            for j in range(0, SPAN, 2)
        ],
        axis=1,
    ).astype(BF16)
    flat_v = jnp.concatenate(
        [
            jnp.where(low8, pltpu.roll(steps[j], HEAD_DIM, 1), steps[j + 1])
            for j in range(0, SPAN, 2)
        ],
        axis=1,
    ).astype(BF16)
    kin_c.wait()
    vin_c.wait()
    kout_c.wait()
    vout_c.wait()
    hidden_k = jax.nn.gelu(dot_t(flat_k, kin[...])).astype(BF16)
    hidden_v = jax.nn.gelu(dot_t(flat_v, vin[...])).astype(BF16)
    sum_k = dot(hidden_k, kout[...]).astype(BF16).astype(F32)
    sum_v = dot(hidden_v, vout[...]).astype(BF16).astype(F32)

    def sum_slot(index):
        return sums.at[pl.ds(pl.multiple_of(index * runs, runs), runs), :]

    sums[pl.ds(pl.multiple_of(me * runs, runs), runs), :] = jnp.concatenate([sum_k, sum_v], axis=1)

    def sum_copy(source, target):
        return pltpu.make_async_remote_copy(
            src_ref=sum_slot(source),
            dst_ref=sum_slot(source),
            send_sem=send_s.at[target],
            recv_sem=recv_s.at[source],
            device_id={"kv": target},
            device_id_type=MESH,
        )

    lax.fori_loop(jnp.minimum(z + 2, outer), jnp.minimum(z + 3, outer), z_send, 0)

    qw_c.wait()
    queries = dot(tok[...], qw[...]) * (HEAD_DIM**-0.5 * LOG2E)
    lax.fori_loop(jnp.minimum(z + 3, outer), outer, z_send, 0)

    def sum_send(target, carry):
        other = lax.rem(target, inner) != y

        @pl.when(other & ((target != me + 1) | (y != 0)))
        def _():
            wait_ready(target)

        sum_copy(me, target).start()
        return carry

    lax.fori_loop(me + 1, n_kv, sum_send, 0)

    low64 = low_half((HEAD_DIM, LANES))
    for b in range(0, blocks, 2):
        for p in range(pairs):
            lanes = slice(p * LANES, (p + 1) * LANES)
            turned = queries[b * BLOCK : (b + 2) * BLOCK, lanes].T
            even, odd = turned[:HEAD_DIM], turned[HEAD_DIM:]
            stacked[b, :HEAD_DIM, lanes] = jnp.where(
                low64, even, pltpu.roll(odd, BLOCK, 1)
            ).astype(BF16)
            stacked[b + 1, :HEAD_DIM, lanes] = jnp.where(
                low64, pltpu.roll(even, BLOCK, 1), odd
            ).astype(BF16)
        stacked[b, HEAD_DIM:, :] = jnp.zeros((HEAD_DIM, cols), BF16)
        stacked[b + 1, HEAD_DIM:, :] = jnp.zeros((HEAD_DIM, cols), BF16)
    gw_c.wait()
    gates = jax.nn.sigmoid(dot_t(gw[...], tok[...]))
    half = gates.shape[0] // 2
    low1 = low_half((1, LANES))
    for branch in range(2):
        at = branch * half
        mine = jnp.where(g == 0, gates[at : at + heads], gates[at + heads : at + 2 * heads])
        for b in range(blocks):
            here = mine[:, b // 2 * LANES : (b // 2 + 1) * LANES]
            moved = pltpu.roll(here, BLOCK, 1)
            left, right = (here, moved) if b % 2 == 0 else (moved, here)
            gate_rows[pl.ds(branch * blocks + b, 1), :] = jnp.concatenate(
                [
                    jnp.where(low1, left[2 * p : 2 * p + 1], right[2 * p + 1 : 2 * p + 2])
                    for p in range(pairs)
                ],
                axis=1,
            )

    def forward(step, carry):
        is_first = jnp.int32(step == 1)
        source = is_first * (z - 1) + (1 - is_first) * (step - 2)
        for part in range(PARTS):
            z_copy(source, z, part).wait_recv()
            if inner == 2:
                y_copy(source, y, part).start()
        return carry

    lax.fori_loop(1, z + 1, forward, 0)

    def sum_wait(source, carry):
        sum_copy(source, me).wait_recv()
        return carry

    lax.fori_loop(0, me, sum_wait, 0)
    sums_kv = sums[...].astype(BF16)
    total_runs = sums_kv.shape[0]
    low_runs = low_half((total_runs, LANES))
    sums_1v = jnp.where(low_runs, jnp.ones_like(sums_kv), sums_kv)
    row_in = lax.rem(lax.broadcasted_iota(jnp.int32, (1, cols), 1), BLOCK)
    run_end = lax.broadcasted_iota(jnp.int32, (total_runs, 1), 0) * SPAN + SPAN - 1
    for b in range(blocks):
        allowed = run_end <= me * local + b * BLOCK + row_in
        shifted = jnp.where(allowed, dot(sums_kv, stacked[b]), -1e30)
        top = jnp.max(shifted, axis=0, keepdims=True)
        weights = jnp.where(allowed, jnp.exp2(shifted - top), 0.0).astype(BF16)
        o_s = dot_rows(sums_1v, weights)
        scale = gate_rows[pl.ds(b, 1), :] / jnp.maximum(o_s[:1], 1.0)
        summary_mix[b] = o_s[HEAD_DIM:] * scale

    sel_c.wait()
    ow_c.wait()
    if inner == 2:

        def y_wait(step, carry):
            for part in range(PARTS):
                y_copy(z - step, 1 - y, part).wait_recv()
            return carry

        lax.fori_loop(1 - y, z + 1, y_wait, 0)

    key_in = lax.broadcasted_iota(jnp.int32, (BLOCK, 1), 0)
    own_allowed = key_in <= row_in
    low_keys = low_half((picks * BLOCK, LANES))
    mixes = []
    for b in range(blocks):
        rows = slice(b * BLOCK, (b + 1) * BLOCK)
        chosen = [sel[0, b, s] for s in range(picks)]
        kv = jnp.concatenate([gathered[jnp.maximum(c, 0)] for c in chosen], axis=0)
        raw = dot(kv, stacked[b])
        scores = jnp.concatenate(
            [jnp.where(own_allowed, raw[:BLOCK], -1e30)]
            + [
                raw[s * BLOCK : (s + 1) * BLOCK] + jnp.where(chosen[s] >= 0, 0.0, -1e30)
                for s in range(1, picks)
            ],
            axis=0,
        )
        top = jnp.max(scores, axis=0, keepdims=True)
        weights = jnp.exp2(scores - top).astype(BF16)
        o_c = dot_rows(jnp.where(low_keys, jnp.ones_like(kv), kv), weights)
        scale = gate_rows[pl.ds(blocks + b, 1), :] / o_c[:1]
        mixed = summary_mix[b] + o_c[HEAD_DIM:] * scale
        for p in range(0, pairs, 2):
            one = mixed[:, p * LANES : (p + 1) * LANES]
            two = mixed[:, (p + 1) * LANES : (p + 2) * LANES]
            turned = jnp.concatenate(
                [
                    jnp.where(low64, one, pltpu.roll(two, BLOCK, 1)),
                    jnp.where(low64, pltpu.roll(one, BLOCK, 1), two),
                ],
                axis=0,
            ).T.astype(BF16)
            own_mix[rows, p * LANES : (p + 1) * LANES] = turned[:BLOCK]
            own_mix[rows, (p + 1) * LANES : (p + 2) * LANES] = turned[BLOCK:]
        mix = pltpu.make_async_remote_copy(
            src_ref=own_mix.at[rows],
            dst_ref=peer_mix.at[rows],
            send_sem=send_m.at[b],
            recv_sem=recv_m.at[b],
            device_id={"tp": 1 - g},
            device_id_type=MESH,
        )
        mix.start()
        mixes.append(mix)

    own_rows = pl.ds(pl.multiple_of(g * cols, cols), cols)
    peer_rows = pl.ds(pl.multiple_of((1 - g) * cols, cols), cols)
    partial[...] = dot(own_mix[...], ow[own_rows, :])
    for mix in mixes:
        mix.wait_recv()
    out_ref[...] = (partial[...] + dot(peer_mix[...], ow[peer_rows, :])).astype(BF16)
    for mix in mixes:
        mix.wait_send()

    def z_done(target, carry):
        for part in range(PARTS):
            z_copy(z, target, part).wait_send()
        return carry

    lax.fori_loop(z + 1, outer, z_done, 0)

    def sum_done(target, carry):
        sum_copy(me, target).wait_send()
        return carry

    lax.fori_loop(me + 1, n_kv, sum_done, 0)
    if inner == 2:

        def y_done(step, carry):
            for part in range(PARTS):
                y_copy(z - step, y, part).wait_send()
            return carry

        lax.fori_loop(y, z + 1, y_done, 0)


def per_device(n_kv, tokens, qw, kw, vw, gw, kin, kout, vin, vout, ow, selection):
    gw, kin, vin = gw.T, kin.T, vin.T
    local, width = tokens.shape
    cols = qw.shape[1]
    inner = 2 if n_kv % 2 == 0 else 1
    outer = n_kv // inner
    blocks = local // BLOCK
    runs = local // SPAN
    hbm = pl.BlockSpec(memory_space=pltpu.HBM)
    dma = pltpu.SemaphoreType.DMA
    vm = pltpu.VMEM
    operands = [
        pltpu.with_memory_space_constraint(a, pltpu.HBM)
        for a in (selection, tokens, qw, kw, vw, gw, kin, kout, vin, vout, ow)
    ]
    return pl.pallas_call(
        functools.partial(kernel, n_kv, inner),
        out_shape=pltpu.VMEM((local, ow.shape[1]), BF16),
        in_specs=[hbm] * 11,
        out_specs=pl.BlockSpec(memory_space=pltpu.VMEM),
        scratch_shapes=[
            pltpu.SMEM(selection.shape, jnp.int32),
            vm(tokens.shape, BF16),
            vm(qw.shape, BF16),
            vm((width, 2 * LANES), BF16),
            vm(gw.shape, BF16),
            vm(kin.shape, BF16),
            vm(kout.shape, BF16),
            vm(vin.shape, BF16),
            vm(vout.shape, BF16),
            vm(ow.shape, BF16),
            vm((local, LANES), F32),
            vm((n_kv * blocks, BLOCK, LANES), BF16),
            vm((n_kv * runs, LANES), F32),
            vm((blocks, LANES, cols), BF16),
            vm((blocks, HEAD_DIM, cols), F32),
            vm((2 * blocks, cols), F32),
            vm((local, cols), BF16),
            vm((local, cols), BF16),
            vm((local, ow.shape[1]), F32),
            dma((3 * CHUNKS + 8,)),
            pltpu.SemaphoreType.REGULAR((n_kv,)),
            dma((outer, PARTS)),
            dma((outer, PARTS)),
            dma((outer, PARTS)),
            dma((outer, PARTS)),
            dma((n_kv,)),
            dma((n_kv,)),
            dma((blocks,)),
            dma((blocks,)),
        ],
        compiler_params=pltpu.CompilerParams(
            collective_id=0, has_side_effects=True, vmem_limit_bytes=GRANT
        ),
        name="attend",
    )(*operands)


def solution(mesh):
    in_specs = (
        P(("dp", "kv"), None),
        P(None, "tp"),
        P(),
        P(),
        P(),
        P(),
        P(),
        P(),
        P(),
        P(None, "tp"),
        P("tp", ("dp", "kv"), None),
    )
    out_specs = P(("dp", "kv"), "tp")
    return jax.shard_map(
        functools.partial(per_device, mesh.shape["kv"]),
        mesh=mesh,
        in_specs=in_specs,
        out_specs=out_specs,
        check_vma=False,
    )
```

```python
import functools

import jax
import jax.numpy as jnp
from jax import lax
from jax.experimental import pallas as pl
from jax.experimental.pallas import tpu as pltpu
from jax.sharding import PartitionSpec as P

HEAD_DIM = 64
BLOCK = 64
SPAN = 32
LANES = 128
MESH = pl.DeviceIdType.MESH
F32 = jnp.float32
BF16 = jnp.bfloat16
CHUNKS = 4
PARTS = 2
AHEAD = 8
LOG2E = 1.4426950408889634
GRANT = 40 * 1024 * 1024


def dot(a, b):
    return jnp.dot(a, b, preferred_element_type=F32)


def dot_t(a, b):
    return lax.dot_general(a, b, (((1,), (1,)), ((), ())), preferred_element_type=F32)


def low_half(shape):
    return lax.broadcasted_iota(jnp.int32, shape, len(shape) - 1) < HEAD_DIM


def kernel(
    n_kv,
    inner,
    sel_hbm,
    tok_hbm,
    qw_hbm,
    kw_hbm,
    vw_hbm,
    gw_hbm,
    kin_hbm,
    kout_hbm,
    vin_hbm,
    vout_hbm,
    ow_hbm,
    out_ref,
    sel,
    tok,
    qw,
    kvw,
    gw,
    kin,
    kout,
    vin,
    vout,
    ow,
    rows32,
    gathered,
    sums,
    stacked,
    summary_mix,
    gate_wide,
    own_mix,
    peer_mix,
    partial,
    load_sem,
    ready,
    send_z,
    recv_z,
    send_y,
    recv_y,
    send_s,
    recv_s,
    send_m,
    recv_m,
):
    local, width = tok.shape
    runs = local // SPAN
    blocks = local // BLOCK
    cols = qw.shape[1]
    heads = cols // HEAD_DIM
    pairs = cols // LANES
    picks = sel.shape[2]
    outer = n_kv // inner
    me = lax.axis_index("kv")
    g = lax.axis_index("tp")
    z = me // inner
    y = lax.rem(me, inner)

    barrier = pltpu.get_barrier_semaphore()

    def greet(target, carry):
        pl.semaphore_signal(barrier, inc=1, device_id={"kv": target}, device_id_type=MESH)
        return carry

    lax.fori_loop(me + 1, n_kv, greet, 0)
    pl.semaphore_signal(barrier, inc=1, device_id={"tp": 1 - g}, device_id_type=MESH)

    depth = width // CHUNKS
    first = []
    for c in range(CHUNKS):
        part = pl.ds(c * depth, depth)
        trio = [
            pltpu.make_async_copy(tok_hbm.at[:, part], tok.at[:, part], load_sem.at[3 * c]),
            pltpu.make_async_copy(
                kw_hbm.at[part], kvw.at[part, pl.ds(0, LANES)], load_sem.at[3 * c + 1]
            ),
            pltpu.make_async_copy(
                vw_hbm.at[part], kvw.at[part, pl.ds(LANES, LANES)], load_sem.at[3 * c + 2]
            ),
        ]
        for copy in trio:
            copy.start()
        first.append(trio)
    base = 3 * CHUNKS
    later = [
        pltpu.make_async_copy(src, dst, load_sem.at[base + i])
        for i, (src, dst) in enumerate(
            [
                (kin_hbm, kin),
                (vin_hbm, vin),
                (kout_hbm, kout),
                (vout_hbm, vout),
                (qw_hbm, qw),
                (gw_hbm, gw),
                (sel_hbm, sel),
                (ow_hbm, ow),
            ]
        )
    ]
    kin_c, vin_c, kout_c, vout_c, qw_c, gw_c, sel_c, ow_c = later

    sums[...] = jnp.zeros_like(sums)
    pl.semaphore_wait(barrier, me + 1)

    def tell(target, carry):
        pl.semaphore_signal(ready.at[me], inc=1, device_id={"kv": target}, device_id_type=MESH)
        return carry

    lax.fori_loop(0, me, tell, 0)

    acc = jnp.zeros((local, 2 * LANES), F32)
    for c in range(CHUNKS):
        for copy in first[c]:
            copy.wait()
        if c == CHUNKS - 2:
            for copy in later:
                copy.start()
        part = pl.ds(c * depth, depth)
        acc += dot(tok[:, part], kvw[part, :])
    keys = acc[:, :LANES]
    values = acc[:, LANES:]
    low = low_half((local, LANES))
    paired = jnp.where(
        g == 0,
        jnp.where(low, keys, pltpu.roll(values, HEAD_DIM, 1)),
        jnp.where(low, pltpu.roll(keys, HEAD_DIM, 1), values),
    ).astype(BF16)
    gathered[pl.ds(me * blocks, blocks)] = paired.reshape(blocks, BLOCK, LANES)
    rows32[...] = paired.astype(F32)

    part_blocks = blocks // PARTS

    def slot(index, part):
        return gathered.at[pl.ds(index * blocks + part * part_blocks, part_blocks)]

    def z_copy(source_z, target_z, part):
        return pltpu.make_async_remote_copy(
            src_ref=slot(source_z * inner + y, part),
            dst_ref=slot(source_z * inner + y, part),
            send_sem=send_z.at[target_z, part],
            recv_sem=recv_z.at[source_z, part],
            device_id={"kv": target_z * inner + y},
            device_id_type=MESH,
        )

    def y_copy(source_z, source_y, part):
        return pltpu.make_async_remote_copy(
            src_ref=slot(source_z * inner + source_y, part),
            dst_ref=slot(source_z * inner + source_y, part),
            send_sem=send_y.at[source_z, part],
            recv_sem=recv_y.at[source_z, part],
            device_id={"kv": z * inner + lax.rem(y + 1, inner)},
            device_id_type=MESH,
        )

    def wait_ready(index):
        pl.semaphore_wait(ready.at[index], 1)

    def z_send(target, carry):
        wait_ready(target * inner + y)
        for part in range(PARTS):
            z_copy(z, target, part).start()
        return carry

    lax.fori_loop(z + 1, jnp.minimum(z + 2, outer), z_send, 0)
    if inner == 2:

        @pl.when(y == 0)
        def _():
            wait_ready(me + 1)
            for part in range(PARTS):
                y_copy(z, 0, part).start()

    steps = [rows32[pl.ds(j, runs, stride=SPAN), :] for j in range(SPAN)]
    low8 = low_half((runs, LANES))
    flat_k = jnp.concatenate(
        [
            jnp.where(low8, steps[j], pltpu.roll(steps[j + 1], HEAD_DIM, 1))
            for j in range(0, SPAN, 2)
        ],
        axis=1,
    ).astype(BF16)
    flat_v = jnp.concatenate(
        [
            jnp.where(low8, pltpu.roll(steps[j], HEAD_DIM, 1), steps[j + 1])
            for j in range(0, SPAN, 2)
        ],
        axis=1,
    ).astype(BF16)
    kin_c.wait()
    vin_c.wait()
    kout_c.wait()
    vout_c.wait()
    hidden_k = jax.nn.gelu(dot_t(flat_k, kin[...])).astype(BF16)
    hidden_v = jax.nn.gelu(dot_t(flat_v, vin[...])).astype(BF16)
    sum_k = dot(hidden_k, kout[...]).astype(BF16).astype(F32)
    sum_v = dot(hidden_v, vout[...]).astype(BF16).astype(F32)

    def sum_slot(index):
        return sums.at[pl.ds(pl.multiple_of(index * runs, runs), runs), :]

    sums[pl.ds(pl.multiple_of(me * runs, runs), runs), :] = jnp.concatenate([sum_k, sum_v], axis=1)

    def sum_copy(source, target):
        return pltpu.make_async_remote_copy(
            src_ref=sum_slot(source),
            dst_ref=sum_slot(source),
            send_sem=send_s.at[target],
            recv_sem=recv_s.at[source],
            device_id={"kv": target},
            device_id_type=MESH,
        )

    lax.fori_loop(jnp.minimum(z + 2, outer), jnp.minimum(z + 3, outer), z_send, 0)

    qw_c.wait()
    queries = dot(tok[...], qw[...]) * (HEAD_DIM**-0.5 * LOG2E)
    lax.fori_loop(jnp.minimum(z + 3, outer), outer, z_send, 0)

    def sum_send(target, carry):
        other = lax.rem(target, inner) != y

        @pl.when(other & ((target != me + 1) | (y != 0)))
        def _():
            wait_ready(target)

        sum_copy(me, target).start()
        return carry

    lax.fori_loop(me + 1, n_kv, sum_send, 0)

    low64 = low_half((BLOCK, LANES))
    row_in = lax.broadcasted_iota(jnp.int32, (BLOCK, 1), 0)
    lane = lax.broadcasted_iota(jnp.int32, (1, LANES), 1)
    unit = jnp.where(lane - HEAD_DIM == row_in, 1.0, 0.0)
    for b in range(blocks):
        rows = slice(b * BLOCK, (b + 1) * BLOCK)
        for p in range(pairs):
            two = queries[rows, p * LANES : (p + 1) * LANES]
            at = 2 * p * BLOCK
            stacked[b, at : at + BLOCK] = jnp.where(low64, two, unit).astype(BF16)
            stacked[b, at + BLOCK : at + 2 * BLOCK] = jnp.where(
                low64, pltpu.roll(two, HEAD_DIM, 1), unit
            ).astype(BF16)
    gw_c.wait()
    gates = jax.nn.sigmoid(dot_t(tok[...], gw[...]))
    half = gates.shape[1] // 2
    gate_s = jnp.where(g == 0, gates[:, :heads], gates[:, heads:half])
    gate_c = jnp.where(g == 0, gates[:, half : half + heads], gates[:, half + heads :])
    for b in range(blocks):
        rows = slice(b * BLOCK, (b + 1) * BLOCK)
        for h in range(heads):
            at = slice(h * BLOCK, (h + 1) * BLOCK)
            gate_wide[b, at] = jnp.broadcast_to(gate_c[rows, h : h + 1], (BLOCK, LANES))
            summary_mix[b, at] = jnp.broadcast_to(gate_s[rows, h : h + 1], (BLOCK, LANES))

    def forward(step, carry):
        is_first = jnp.int32(step == 1)
        source = is_first * (z - 1) + (1 - is_first) * (step - 2)
        for part in range(PARTS):
            z_copy(source, z, part).wait_recv()
            if inner == 2:
                y_copy(source, y, part).start()
        return carry

    lax.fori_loop(1, z + 1, forward, 0)

    def sum_wait(source, carry):
        sum_copy(source, me).wait_recv()
        return carry

    lax.fori_loop(0, me, sum_wait, 0)
    sums_kv = sums[...].astype(BF16)
    total_runs = sums_kv.shape[0]
    low_runs = low_half((total_runs, LANES))
    sums_1 = jnp.concatenate([sums_kv, jnp.ones_like(sums_kv)], axis=1)
    run_end = lax.broadcasted_iota(jnp.int32, (total_runs, 1), 0) * SPAN + SPAN - 1
    tall_row = lax.rem(lax.broadcasted_iota(jnp.int32, (heads * BLOCK, 1), 0), BLOCK)
    for b in range(blocks):
        first_row = me * local + b * BLOCK
        barred = jnp.where(run_end <= first_row + lane - HEAD_DIM, 0.0, -1e30).astype(BF16)
        scores = dot_t(stacked[b], jnp.where(low_runs, sums_kv, barred))
        top = jnp.max(scores, axis=1, keepdims=True)
        weights = jnp.exp2(scores - top).astype(BF16)
        o_s = dot(weights, sums_1)
        part = summary_mix[b] * o_s[:, :LANES] / o_s[:, LANES:]
        summary_mix[b] = jnp.where(first_row + tall_row >= SPAN - 1, part, 0.0)

    sel_c.wait()
    ow_c.wait()
    if inner == 2:

        def y_wait(step, carry):
            for part in range(PARTS):
                y_copy(z - step, 1 - y, part).wait_recv()
            return carry

        lax.fori_loop(1 - y, z + 1, y_wait, 0)

    later_key = jnp.where(row_in <= lane - HEAD_DIM, 0.0, -1e30).astype(BF16)
    tall = 2 * LANES
    pieces = [(b, c) for b in range(blocks) for c in range(cols // tall)]
    left, right = {}, {}

    def scores_of(b, c):
        if c == 0:
            score_rows, value_rows = [], []
            for s in range(picks):
                index = sel[0, b, s]
                kv = gathered[jnp.maximum(index, 0)]
                bar = later_key
                if s > 0:
                    bar = jnp.full((BLOCK, LANES), jnp.where(index >= 0, 0.0, -1e30), F32)
                    bar = bar.astype(BF16)
                score_rows.append(jnp.where(low64, kv, bar))
                value_rows.append(kv)
            left[b] = jnp.concatenate(score_rows, axis=0)
            kv = jnp.concatenate(value_rows, axis=0)
            right[b] = jnp.concatenate([kv, jnp.ones_like(kv)], axis=1)
        return dot_t(stacked[b, c * tall : (c + 1) * tall, :], left[b])

    mixes = []
    queue = [scores_of(*piece) for piece in pieces[:AHEAD]]
    for i, (b, c) in enumerate(pieces):
        rows = slice(b * BLOCK, (b + 1) * BLOCK)
        at = slice(c * tall, (c + 1) * tall)
        scores = queue.pop(0)
        if i + AHEAD < len(pieces):
            queue.append(scores_of(*pieces[i + AHEAD]))
        top = jnp.max(scores, axis=1, keepdims=True)
        weights = jnp.exp2(scores - top).astype(BF16)
        o_c = dot(weights, right[b])
        mixed = summary_mix[b, at] + gate_wide[b, at] * (o_c[:, :LANES] / o_c[:, LANES:])
        for p in range(tall // LANES):
            even = mixed[2 * p * BLOCK : (2 * p + 1) * BLOCK]
            odd_head = mixed[(2 * p + 1) * BLOCK : (2 * p + 2) * BLOCK]
            here = (c * tall // LANES + p) * LANES
            own_mix[rows, here : here + LANES] = jnp.where(
                low64, pltpu.roll(even, HEAD_DIM, 1), odd_head
            ).astype(BF16)
        if c < cols // tall - 1:
            continue
        mix = pltpu.make_async_remote_copy(
            src_ref=own_mix.at[rows],
            dst_ref=peer_mix.at[rows],
            send_sem=send_m.at[b],
            recv_sem=recv_m.at[b],
            device_id={"tp": 1 - g},
            device_id_type=MESH,
        )
        mix.start()
        mixes.append(mix)

    own_rows = pl.ds(pl.multiple_of(g * cols, cols), cols)
    peer_rows = pl.ds(pl.multiple_of((1 - g) * cols, cols), cols)
    partial[...] = dot(own_mix[...], ow[own_rows, :])
    for mix in mixes:
        mix.wait_recv()
    out_ref[...] = (partial[...] + dot(peer_mix[...], ow[peer_rows, :])).astype(BF16)
    for mix in mixes:
        mix.wait_send()

    def z_done(target, carry):
        for part in range(PARTS):
            z_copy(z, target, part).wait_send()
        return carry

    lax.fori_loop(z + 1, outer, z_done, 0)

    def sum_done(target, carry):
        sum_copy(me, target).wait_send()
        return carry

    lax.fori_loop(me + 1, n_kv, sum_done, 0)
    if inner == 2:

        def y_done(step, carry):
            for part in range(PARTS):
                y_copy(z - step, y, part).wait_send()
            return carry

        lax.fori_loop(y, z + 1, y_done, 0)


def per_device(n_kv, tokens, qw, kw, vw, gw, kin, kout, vin, vout, ow, selection):
    gw, kin, vin = gw.T, kin.T, vin.T
    local, width = tokens.shape
    cols = qw.shape[1]
    inner = 2 if n_kv % 2 == 0 else 1
    outer = n_kv // inner
    blocks = local // BLOCK
    runs = local // SPAN
    tall = cols // HEAD_DIM * BLOCK
    hbm = pl.BlockSpec(memory_space=pltpu.HBM)
    dma = pltpu.SemaphoreType.DMA
    vm = pltpu.VMEM
    operands = [
        pltpu.with_memory_space_constraint(a, pltpu.HBM)
        for a in (selection, tokens, qw, kw, vw, gw, kin, kout, vin, vout, ow)
    ]
    return pl.pallas_call(
        functools.partial(kernel, n_kv, inner),
        out_shape=pltpu.VMEM((local, ow.shape[1]), BF16),
        in_specs=[hbm] * 11,
        out_specs=pl.BlockSpec(memory_space=pltpu.VMEM),
        scratch_shapes=[
            pltpu.SMEM(selection.shape, jnp.int32),
            vm(tokens.shape, BF16),
            vm(qw.shape, BF16),
            vm((width, 2 * LANES), BF16),
            vm(gw.shape, BF16),
            vm(kin.shape, BF16),
            vm(kout.shape, BF16),
            vm(vin.shape, BF16),
            vm(vout.shape, BF16),
            vm(ow.shape, BF16),
            vm((local, LANES), F32),
            vm((n_kv * blocks, BLOCK, LANES), BF16),
            vm((n_kv * runs, LANES), F32),
            vm((blocks, tall, LANES), BF16),
            vm((blocks, tall, LANES), F32),
            vm((blocks, tall, LANES), F32),
            vm((local, cols), BF16),
            vm((local, cols), BF16),
            vm((local, ow.shape[1]), F32),
            dma((3 * CHUNKS + 8,)),
            pltpu.SemaphoreType.REGULAR((n_kv,)),
            dma((outer, PARTS)),
            dma((outer, PARTS)),
            dma((outer, PARTS)),
            dma((outer, PARTS)),
            dma((n_kv,)),
            dma((n_kv,)),
            dma((blocks,)),
            dma((blocks,)),
        ],
        compiler_params=pltpu.CompilerParams(
            collective_id=0, has_side_effects=True, vmem_limit_bytes=GRANT
        ),
        name="attend",
    )(*operands)


def solution(mesh):
    in_specs = (
        P(("dp", "kv"), None),
        P(None, "tp"),
        P(),
        P(),
        P(),
        P(),
        P(),
        P(),
        P(),
        P(None, "tp"),
        P("tp", ("dp", "kv"), None),
    )
    out_specs = P(("dp", "kv"), "tp")
    return jax.shard_map(
        functools.partial(per_device, mesh.shape["kv"]),
        mesh=mesh,
        in_specs=in_specs,
        out_specs=out_specs,
        check_vma=False,
    )
```

```python
import functools

import jax
import jax.numpy as jnp
from jax import lax
from jax.experimental import pallas as pl
from jax.experimental.pallas import tpu as pltpu
from jax.sharding import PartitionSpec as P

HEAD_DIM = 64
BLOCK = 64
SPAN = 32
LANES = 128
MESH = pl.DeviceIdType.MESH
F32 = jnp.float32
BF16 = jnp.bfloat16
CHUNKS = 4
PARTS = 4
SEND_ORDER = ((0, 0, 1), (0, 0, 4))
AHEAD = 8
LOG2E = 1.4426950408889634
GRANT = 40 * 1024 * 1024


def dot(a, b):
    return jnp.dot(a, b, preferred_element_type=F32)


def dot_t(a, b):
    return lax.dot_general(a, b, (((1,), (1,)), ((), ())), preferred_element_type=F32)


def low_half(shape):
    return lax.broadcasted_iota(jnp.int32, shape, len(shape) - 1) < HEAD_DIM


def kernel(
    n_kv,
    inner,
    sel_hbm,
    tok_hbm,
    qw_hbm,
    kw_hbm,
    vw_hbm,
    gw_hbm,
    kin_hbm,
    kout_hbm,
    vin_hbm,
    vout_hbm,
    ow_hbm,
    out_ref,
    sel,
    tok,
    qw,
    kvw,
    gw,
    kin,
    kout,
    vin,
    vout,
    ow,
    rows32,
    gathered,
    sums,
    stacked,
    summary_mix,
    gate_wide,
    own_mix,
    peer_mix,
    partial,
    load_sem,
    ready,
    send_z,
    recv_z,
    send_y,
    recv_y,
    send_s,
    recv_s,
    send_m,
    recv_m,
):
    local, width = tok.shape
    runs = local // SPAN
    blocks = local // BLOCK
    cols = qw.shape[1]
    heads = cols // HEAD_DIM
    pairs = cols // LANES
    picks = sel.shape[2]
    outer = n_kv // inner
    me = lax.axis_index("kv")
    g = lax.axis_index("tp")
    z = me // inner
    y = lax.rem(me, inner)

    sums[...] = jnp.zeros_like(sums)
    barrier = pltpu.get_barrier_semaphore()

    def greet(target, carry):
        pl.semaphore_signal(
            barrier, inc=1, device_id={"kv": target * inner + y}, device_id_type=MESH
        )
        return carry

    def partner():
        return {"kv": z * inner + lax.rem(y + 1, inner)}

    lax.fori_loop(z + 1, outer, greet, 0)
    if inner == 2:

        @pl.when(y == 0)
        def _():
            pl.semaphore_signal(barrier, inc=1, device_id=partner(), device_id_type=MESH)

    pl.semaphore_signal(barrier, inc=1, device_id={"tp": 1 - g}, device_id_type=MESH)

    depth = width // CHUNKS
    first = []
    for c in range(CHUNKS):
        part = pl.ds(c * depth, depth)
        trio = [
            pltpu.make_async_copy(tok_hbm.at[:, part], tok.at[:, part], load_sem.at[c]),
            pltpu.make_async_copy(
                kw_hbm.at[part], kvw.at[part, pl.ds(0, LANES)], load_sem.at[c]
            ),
            pltpu.make_async_copy(
                vw_hbm.at[part], kvw.at[part, pl.ds(LANES, LANES)], load_sem.at[c]
            ),
        ]
        for copy in trio:
            copy.start()
        first.append(trio)
    base = CHUNKS
    span_rows = depth * (local + 2 * LANES) // (2 * LANES)
    whole_chunk = kvw.at[pl.ds(0, span_rows)]
    later = [
        pltpu.make_async_copy(src, dst, load_sem.at[base + i])
        for i, (src, dst) in enumerate(
            [
                (kin_hbm, kin),
                (vin_hbm, vin),
                (kout_hbm, kout),
                (vout_hbm, vout),
                (qw_hbm, qw),
                (gw_hbm, gw),
                (sel_hbm, sel),
                (ow_hbm, ow),
            ]
        )
    ]
    kin_c, vin_c, kout_c, vout_c, qw_c, gw_c, sel_c, ow_c = later


    pl.semaphore_wait(barrier, z + y + 1)

    def tell(step, carry):
        pl.semaphore_signal(
            ready.at[z], inc=1, device_id={"kv": (z - step) * inner + y}, device_id_type=MESH
        )
        return carry

    lax.fori_loop(1, z + 1, tell, 0)
    if inner == 2:

        @pl.when(y == 1)
        def _():
            pl.semaphore_signal(ready.at[z], inc=1, device_id=partner(), device_id_type=MESH)

    acc = jnp.zeros((local, 2 * LANES), F32)
    for c in range(CHUNKS):
        pltpu.make_async_copy(whole_chunk, whole_chunk, load_sem.at[c]).wait()
        if c == 0:
            for copy in later[:4]:
                copy.start()
        if c == CHUNKS - 2:
            for copy in later[4:]:
                copy.start()
        part = pl.ds(c * depth, depth)
        acc += dot(tok[:, part], kvw[part, :])
    keys = acc[:, :LANES]
    values = acc[:, LANES:]
    low = low_half((local, LANES))
    paired = jnp.where(
        g == 0,
        jnp.where(low, keys, pltpu.roll(values, HEAD_DIM, 1)),
        jnp.where(low, pltpu.roll(keys, HEAD_DIM, 1), values),
    ).astype(BF16)
    gathered[pl.ds(me * blocks, blocks)] = paired.reshape(blocks, BLOCK, LANES)
    rows32[...] = paired.astype(F32)

    part_blocks = blocks // PARTS

    def full(index):
        return gathered.at[pl.ds(index * blocks, blocks)]

    def slot(index, part):
        return gathered.at[pl.ds(index * blocks + part * part_blocks, part_blocks)]

    def z_copy(source_z, target_z, part):
        return pltpu.make_async_remote_copy(
            src_ref=slot(source_z * inner + y, part),
            dst_ref=slot(source_z * inner + y, part),
            send_sem=send_z.at[target_z],
            recv_sem=recv_z.at[source_z, part],
            device_id={"kv": target_z * inner + y},
            device_id_type=MESH,
        )

    def y_copy(source_z, source_y, part):
        return pltpu.make_async_remote_copy(
            src_ref=slot(source_z * inner + source_y, part),
            dst_ref=slot(source_z * inner + source_y, part),
            send_sem=send_y.at[source_z],
            recv_sem=recv_y.at[source_z],
            device_id={"kv": z * inner + lax.rem(y + 1, inner)},
            device_id_type=MESH,
        )

    def z_send(target, carry):
        pl.semaphore_wait(ready.at[target], 1)
        for part in range(PARTS):
            z_copy(z, target, part).start()
        return carry

    def send_near():
        lax.fori_loop(jnp.minimum(z + 1, outer), jnp.minimum(z + 2, outer), z_send, 0)

    def send_far():
        lax.fori_loop(jnp.minimum(z + 2, outer), outer, z_send, 0)

    def send_across():
        if inner == 2:

            @pl.when(y == 0)
            def _():
                pl.semaphore_wait(ready.at[z], 1)
                for part in range(PARTS):
                    y_copy(z, 0, part).start()

    def send_at(point):
        for core, order in enumerate(SEND_ORDER):
            jobs = [job for at, job in zip(order, (send_near, send_across, send_far)) if at == point]
            if jobs:

                @pl.when(g == core)
                def _():
                    for job in jobs:
                        job()

    send_at(0)
    steps = [rows32[pl.ds(j, runs, stride=SPAN), :] for j in range(SPAN)]
    low8 = low_half((runs, LANES))
    flat_k = jnp.concatenate(
        [
            jnp.where(low8, steps[j], pltpu.roll(steps[j + 1], HEAD_DIM, 1))
            for j in range(0, SPAN, 2)
        ],
        axis=1,
    ).astype(BF16)
    flat_v = jnp.concatenate(
        [
            jnp.where(low8, pltpu.roll(steps[j], HEAD_DIM, 1), steps[j + 1])
            for j in range(0, SPAN, 2)
        ],
        axis=1,
    ).astype(BF16)
    kin_c.wait()
    vin_c.wait()
    kout_c.wait()
    vout_c.wait()
    hidden_k = jax.nn.gelu(dot_t(flat_k, kin[...])).astype(BF16)
    hidden_v = jax.nn.gelu(dot_t(flat_v, vin[...])).astype(BF16)
    sum_k = dot(hidden_k, kout[...]).astype(BF16).astype(F32)
    sum_v = dot(hidden_v, vout[...]).astype(BF16).astype(F32)

    mine = pl.ds(pl.multiple_of(me * runs, runs), runs)
    sums[mine, :] = jnp.concatenate([sum_k, sum_v], axis=1)
    yours = pl.ds(pl.multiple_of((z * inner + lax.rem(y + 1, inner)) * runs, runs), runs)

    def sum_swap(slot):
        return pltpu.make_async_remote_copy(
            src_ref=sums.at[slot, :],
            dst_ref=sums.at[slot, :],
            send_sem=send_s.at[z],
            recv_sem=recv_s.at[z],
            device_id=partner(),
            device_id_type=MESH,
        )

    if inner == 2:
        sum_swap(mine).start()

    def sum_copy(source, target):
        both = inner * runs
        slot = sums.at[pl.ds(pl.multiple_of(source * both, both), both), :]
        return pltpu.make_async_remote_copy(
            src_ref=slot,
            dst_ref=slot,
            send_sem=send_s.at[target],
            recv_sem=recv_s.at[source],
            device_id={"kv": target * inner + y},
            device_id_type=MESH,
        )

    send_at(1)

    qw_c.wait()
    queries = dot(tok[...], qw[...]) * (HEAD_DIM**-0.5 * LOG2E)

    send_at(2)
    low64 = low_half((BLOCK, LANES))
    row_in = lax.broadcasted_iota(jnp.int32, (BLOCK, 1), 0)
    lane = lax.broadcasted_iota(jnp.int32, (1, LANES), 1)
    unit = jnp.where(lane - HEAD_DIM == row_in, 1.0, 0.0)
    for b in range(blocks):
        rows = slice(b * BLOCK, (b + 1) * BLOCK)
        for p in range(pairs):
            two = queries[rows, p * LANES : (p + 1) * LANES]
            at = 2 * p * BLOCK
            stacked[b, at : at + BLOCK] = jnp.where(low64, two, unit).astype(BF16)
            stacked[b, at + BLOCK : at + 2 * BLOCK] = jnp.where(
                low64, pltpu.roll(two, HEAD_DIM, 1), unit
            ).astype(BF16)
    send_at(3)
    gw_c.wait()
    gates = jax.nn.sigmoid(dot_t(tok[...], gw[...]))
    half = gates.shape[1] // 2
    gate_s = jnp.where(g == 0, gates[:, :heads], gates[:, heads:half])
    gate_c = jnp.where(g == 0, gates[:, half : half + heads], gates[:, half + heads :])
    for b in range(blocks):
        rows = slice(b * BLOCK, (b + 1) * BLOCK)
        for h in range(heads):
            at = slice(h * BLOCK, (h + 1) * BLOCK)
            gate_wide[b, at] = jnp.broadcast_to(gate_c[rows, h : h + 1], (BLOCK, LANES))
            summary_mix[b, at] = jnp.broadcast_to(gate_s[rows, h : h + 1], (BLOCK, LANES))

    def sum_send(target, carry):
        sum_copy(z, target).start()
        return carry

    send_at(4)
    if inner == 2:
        sum_swap(yours).wait_recv()
    lax.fori_loop(z + 1, outer, sum_send, 0)

    def forward(step, carry):
        is_first = jnp.int32(step == 1)
        source = is_first * (z - 1) + (1 - is_first) * (step - 2)
        for part in range(PARTS):
            z_copy(source, z, part).wait_recv()
            if inner == 2:
                y_copy(source, y, part).start()
        return carry

    lax.fori_loop(1, z + 1, forward, 0)

    def sum_wait(source, carry):
        sum_copy(source, z).wait_recv()
        return carry

    lax.fori_loop(0, z, sum_wait, 0)
    sums_kv = sums[...].astype(BF16)
    total_runs = sums_kv.shape[0]
    low_runs = low_half((total_runs, LANES))
    sums_1 = jnp.concatenate([sums_kv, jnp.ones_like(sums_kv)], axis=1)
    run_end = lax.broadcasted_iota(jnp.int32, (total_runs, 1), 0) * SPAN + SPAN - 1
    tall_row = lax.rem(lax.broadcasted_iota(jnp.int32, (heads * BLOCK, 1), 0), BLOCK)
    for b in range(blocks):
        first_row = me * local + b * BLOCK
        barred = jnp.where(run_end <= first_row + lane - HEAD_DIM, 0.0, -1e30).astype(BF16)
        scores = dot_t(stacked[b], jnp.where(low_runs, sums_kv, barred))
        top = jnp.max(scores, axis=1, keepdims=True)
        weights = jnp.exp2(scores - top).astype(BF16)
        o_s = dot(weights, sums_1)
        part = summary_mix[b] * o_s[:, :LANES] / o_s[:, LANES:]
        summary_mix[b] = jnp.where(first_row + tall_row >= SPAN - 1, part, 0.0)

    sel_c.wait()
    ow_c.wait()
    if inner == 2:

        def y_wait(step, carry):
            pltpu.make_async_copy(full(me), full(me), recv_y.at[z - step]).wait()
            return carry

        lax.fori_loop(1 - y, z + 1, y_wait, 0)

    later_key = jnp.where(row_in <= lane - HEAD_DIM, 0.0, -1e30).astype(BF16)
    tall = 2 * LANES
    pieces = [(b, c) for b in range(blocks) for c in range(cols // tall)]
    left, right = {}, {}

    def scores_of(b, c):
        if c == 0:
            score_rows, value_rows = [], []
            for s in range(picks):
                index = sel[0, b, s]
                kv = gathered[jnp.maximum(index, 0)]
                bar = later_key
                if s > 0:
                    bar = jnp.full((BLOCK, LANES), jnp.where(index >= 0, 0.0, -1e30), F32)
                    bar = bar.astype(BF16)
                score_rows.append(jnp.where(low64, kv, bar))
                value_rows.append(kv)
            left[b] = jnp.concatenate(score_rows, axis=0)
            kv = jnp.concatenate(value_rows, axis=0)
            right[b] = jnp.concatenate([kv, jnp.ones_like(kv)], axis=1)
        return dot_t(stacked[b, c * tall : (c + 1) * tall, :], left[b])

    queue = [scores_of(*piece) for piece in pieces[:AHEAD]]
    for i, (b, c) in enumerate(pieces):
        rows = slice(b * BLOCK, (b + 1) * BLOCK)
        at = slice(c * tall, (c + 1) * tall)
        scores = queue.pop(0)
        if i + AHEAD < len(pieces):
            queue.append(scores_of(*pieces[i + AHEAD]))
        top = jnp.max(scores, axis=1, keepdims=True)
        weights = jnp.exp2(scores - top).astype(BF16)
        o_c = dot(weights, right[b])
        mixed = summary_mix[b, at] + gate_wide[b, at] * (o_c[:, :LANES] / o_c[:, LANES:])
        for p in range(tall // LANES):
            even = mixed[2 * p * BLOCK : (2 * p + 1) * BLOCK]
            odd_head = mixed[(2 * p + 1) * BLOCK : (2 * p + 2) * BLOCK]
            here = (c * tall // LANES + p) * LANES
            own_mix[rows, here : here + LANES] = jnp.where(
                low64, pltpu.roll(even, HEAD_DIM, 1), odd_head
            ).astype(BF16)
        if c < cols // tall - 1:
            continue
        mix = pltpu.make_async_remote_copy(
            src_ref=own_mix.at[rows],
            dst_ref=peer_mix.at[rows],
            send_sem=send_m.at[0],
            recv_sem=recv_m.at[0],
            device_id={"tp": 1 - g},
            device_id_type=MESH,
        )
        mix.start()

    own_rows = pl.ds(pl.multiple_of(g * cols, cols), cols)
    peer_rows = pl.ds(pl.multiple_of((1 - g) * cols, cols), cols)
    partial[...] = dot(own_mix[...], ow[own_rows, :])
    all_mixes = pltpu.make_async_remote_copy(
        src_ref=own_mix,
        dst_ref=peer_mix,
        send_sem=send_m.at[0],
        recv_sem=recv_m.at[0],
        device_id={"tp": 1 - g},
        device_id_type=MESH,
    )
    all_mixes.wait_recv()
    out_ref[...] = (partial[...] + dot(peer_mix[...], ow[peer_rows, :])).astype(BF16)
    all_mixes.wait_send()

    def z_done(target, carry):
        pltpu.make_async_copy(full(me), full(me), send_z.at[target]).wait()
        return carry

    lax.fori_loop(z + 1, outer, z_done, 0)

    def sum_done(target, carry):
        sum_copy(z, target).wait_send()
        return carry

    lax.fori_loop(z + 1, outer, sum_done, 0)
    if inner == 2:
        sum_swap(mine).wait_send()

        def y_done(step, carry):
            pltpu.make_async_copy(full(me), full(me), send_y.at[z - step]).wait()
            return carry

        lax.fori_loop(y, z + 1, y_done, 0)


def per_device(n_kv, tokens, qw, kw, vw, gw, kin, kout, vin, vout, ow, selection):
    gw, kin, vin = gw.T, kin.T, vin.T
    local, width = tokens.shape
    cols = qw.shape[1]
    inner = 2 if n_kv % 2 == 0 else 1
    outer = n_kv // inner
    blocks = local // BLOCK
    runs = local // SPAN
    tall = cols // HEAD_DIM * BLOCK
    hbm = pl.BlockSpec(memory_space=pltpu.HBM)
    dma = pltpu.SemaphoreType.DMA
    vm = pltpu.VMEM
    operands = [
        pltpu.with_memory_space_constraint(a, pltpu.HBM)
        for a in (selection, tokens, qw, kw, vw, gw, kin, kout, vin, vout, ow)
    ]
    return pl.pallas_call(
        functools.partial(kernel, n_kv, inner),
        out_shape=pltpu.VMEM((local, ow.shape[1]), BF16),
        in_specs=[hbm] * 11,
        out_specs=pl.BlockSpec(memory_space=pltpu.VMEM),
        scratch_shapes=[
            pltpu.SMEM(selection.shape, jnp.int32),
            vm(tokens.shape, BF16),
            vm(qw.shape, BF16),
            vm((width, 2 * LANES), BF16),
            vm(gw.shape, BF16),
            vm(kin.shape, BF16),
            vm(kout.shape, BF16),
            vm(vin.shape, BF16),
            vm(vout.shape, BF16),
            vm(ow.shape, BF16),
            vm((local, LANES), F32),
            vm((n_kv * blocks, BLOCK, LANES), BF16),
            vm((n_kv * runs, LANES), F32),
            vm((blocks, tall, LANES), BF16),
            vm((blocks, tall, LANES), F32),
            vm((blocks, tall, LANES), F32),
            vm((local, cols), BF16),
            vm((local, cols), BF16),
            vm((local, ow.shape[1]), F32),
            dma((CHUNKS + 8,)),
            pltpu.SemaphoreType.REGULAR((outer,)),
            dma((outer,)),
            dma((outer, PARTS)),
            dma((outer,)),
            dma((outer,)),
            dma((outer,)),
            dma((outer,)),
            dma((1,)),
            dma((1,)),
        ],
        compiler_params=pltpu.CompilerParams(
            collective_id=0, has_side_effects=True, vmem_limit_bytes=GRANT
        ),
        name="attend",
    )(*operands)


def solution(mesh):
    in_specs = (
        P(("dp", "kv"), None),
        P(None, "tp"),
        P(),
        P(),
        P(),
        P(),
        P(),
        P(),
        P(),
        P(None, "tp"),
        P("tp", ("dp", "kv"), None),
    )
    out_specs = P(("dp", "kv"), "tp")
    return jax.shard_map(
        functools.partial(per_device, mesh.shape["kv"]),
        mesh=mesh,
        in_specs=in_specs,
        out_specs=out_specs,
        check_vma=False,
    )
```

```python
import functools

import jax
import jax.numpy as jnp
from jax import lax
from jax.experimental import pallas as pl
from jax.experimental.pallas import tpu as pltpu
from jax.sharding import PartitionSpec as P

HEAD_DIM = 64
BLOCK = 64
SPAN = 32
LANES = 128
MESH = pl.DeviceIdType.MESH
F32 = jnp.float32
BF16 = jnp.bfloat16
CHUNKS = 4
PARTS = 4
SEND_ORDER = ((0, 0, 1), (0, 0, 4))
AHEAD = 8
LOG2E = 1.4426950408889634
GRANT = 40 * 1024 * 1024


def dot(a, b):
    return jnp.dot(a, b, preferred_element_type=F32)


def dot_t(a, b):
    return lax.dot_general(a, b, (((1,), (1,)), ((), ())), preferred_element_type=F32)


def low_half(shape):
    return lax.broadcasted_iota(jnp.int32, shape, len(shape) - 1) < HEAD_DIM


def kernel(
    n_kv,
    inner,
    sel_hbm,
    tok_hbm,
    qw_hbm,
    kw_hbm,
    vw_hbm,
    gw_hbm,
    kin_hbm,
    kout_hbm,
    vin_hbm,
    vout_hbm,
    ow_hbm,
    out_ref,
    sel,
    tok,
    qw,
    kvw,
    gw,
    kin,
    kout,
    vin,
    vout,
    ow,
    rows32,
    gathered,
    sums,
    stacked,
    summary_mix,
    gate_wide,
    own_mix,
    peer_mix,
    partial,
    load_sem,
    ready,
    send_z,
    recv_z,
    send_y,
    recv_y,
    send_w,
    send_s,
    recv_s,
    send_m,
    recv_m,
):
    local, width = tok.shape
    runs = local // SPAN
    blocks = local // BLOCK
    cols = qw.shape[1]
    heads = cols // HEAD_DIM
    pairs = cols // LANES
    picks = sel.shape[2]
    outer = n_kv // inner
    me = lax.axis_index("kv")
    g = lax.axis_index("tp")
    z = me // inner
    y = lax.rem(me, inner)

    sums[...] = jnp.zeros_like(sums)
    barrier = pltpu.get_barrier_semaphore()

    def greet(target, carry):
        pl.semaphore_signal(
            barrier, inc=1, device_id={"kv": target * inner + y}, device_id_type=MESH
        )
        return carry

    def partner():
        return {"kv": z * inner + lax.rem(y + 1, inner)}

    lax.fori_loop(z + 1, outer, greet, 0)
    if inner == 2:

        @pl.when(y == 0)
        def _():
            pl.semaphore_signal(barrier, inc=1, device_id=partner(), device_id_type=MESH)

    pl.semaphore_signal(barrier, inc=1, device_id={"tp": 1 - g}, device_id_type=MESH)

    depth = width // CHUNKS
    first = []
    for c in range(CHUNKS):
        part = pl.ds(c * depth, depth)
        trio = [
            pltpu.make_async_copy(tok_hbm.at[:, part], tok.at[:, part], load_sem.at[c]),
            pltpu.make_async_copy(
                kw_hbm.at[part], kvw.at[part, pl.ds(0, LANES)], load_sem.at[c]
            ),
            pltpu.make_async_copy(
                vw_hbm.at[part], kvw.at[part, pl.ds(LANES, LANES)], load_sem.at[c]
            ),
        ]
        for copy in trio:
            copy.start()
        first.append(trio)
    base = CHUNKS
    span_rows = depth * (local + 2 * LANES) // (2 * LANES)
    whole_chunk = kvw.at[pl.ds(0, span_rows)]
    later = [
        pltpu.make_async_copy(src, dst, load_sem.at[base + i])
        for i, (src, dst) in enumerate(
            [
                (kin_hbm, kin),
                (vin_hbm, vin),
                (kout_hbm, kout),
                (vout_hbm, vout),
                (qw_hbm, qw),
                (gw_hbm, gw),
                (sel_hbm, sel),
                (ow_hbm, ow),
            ]
        )
    ]
    kin_c, vin_c, kout_c, vout_c, qw_c, gw_c, sel_c, ow_c = later


    pl.semaphore_wait(barrier, z + y + 1)

    def tell(step, carry):
        pl.semaphore_signal(
            ready.at[z], inc=1, device_id={"kv": (z - step) * inner + y}, device_id_type=MESH
        )
        return carry

    lax.fori_loop(1, z + 1, tell, 0)
    if inner == 2:

        @pl.when(y == 1)
        def _():
            pl.semaphore_signal(ready.at[z], inc=1, device_id=partner(), device_id_type=MESH)

    acc = jnp.zeros((local, 2 * LANES), F32)
    for c in range(CHUNKS):
        pltpu.make_async_copy(whole_chunk, whole_chunk, load_sem.at[c]).wait()
        if c == 0:
            for copy in later[:4]:
                copy.start()
        if c == CHUNKS - 2:
            for copy in later[4:]:
                copy.start()
        part = pl.ds(c * depth, depth)
        acc += dot(tok[:, part], kvw[part, :])
    keys = acc[:, :LANES]
    values = acc[:, LANES:]
    low = low_half((local, LANES))
    paired = jnp.where(
        g == 0,
        jnp.where(low, keys, pltpu.roll(values, HEAD_DIM, 1)),
        jnp.where(low, pltpu.roll(keys, HEAD_DIM, 1), values),
    ).astype(BF16)
    gathered[pl.ds(me * blocks, blocks)] = paired.reshape(blocks, BLOCK, LANES)
    rows32[...] = paired.astype(F32)

    part_blocks = blocks // PARTS

    def full(index):
        return gathered.at[pl.ds(index * blocks, blocks)]

    def slot(index, part):
        return gathered.at[pl.ds(index * blocks + part * part_blocks, part_blocks)]

    def z_copy(source_z, target_z, part):
        return pltpu.make_async_remote_copy(
            src_ref=slot(source_z * inner + y, part),
            dst_ref=slot(source_z * inner + y, part),
            send_sem=send_z.at[target_z],
            recv_sem=recv_z.at[source_z, part],
            device_id={"kv": target_z * inner + y},
            device_id_type=MESH,
        )

    def y_copy(source_z, source_y, part):
        return pltpu.make_async_remote_copy(
            src_ref=slot(source_z * inner + source_y, part),
            dst_ref=slot(source_z * inner + source_y, part),
            send_sem=send_y.at[source_z],
            recv_sem=recv_y.at[source_z],
            device_id={"kv": z * inner + lax.rem(y + 1, inner)},
            device_id_type=MESH,
        )

    def z_send(target, carry):
        pl.semaphore_wait(ready.at[target], 1)
        for part in range(PARTS):
            z_copy(z, target, part).start()
        return carry

    def send_near():
        lax.fori_loop(jnp.minimum(z + 1, outer), jnp.minimum(z + 2, outer), z_send, 0)

    def send_far():
        @pl.when(z == 0)
        def _():
            lax.fori_loop(min(2, outer), outer, z_send, 0)

    def pass_on(source_z, part):
        return pltpu.make_async_remote_copy(
            src_ref=slot(source_z * inner + y, part),
            dst_ref=slot(source_z * inner + y, part),
            send_sem=send_w.at[source_z],
            recv_sem=recv_z.at[source_z, part],
            device_id={"kv": (z + 1) * inner + y},
            device_id_type=MESH,
        )

    def passes(source_z):
        return (source_z > 0) & (z < outer - 1)

    def send_across():
        if inner == 2:

            @pl.when(y == 0)
            def _():
                pl.semaphore_wait(ready.at[z], 1)
                for part in range(PARTS):
                    y_copy(z, 0, part).start()

    def send_at(point):
        for core, order in enumerate(SEND_ORDER):
            jobs = [job for at, job in zip(order, (send_near, send_across, send_far)) if at == point]
            if jobs:

                @pl.when(g == core)
                def _():
                    for job in jobs:
                        job()

    send_at(0)
    steps = [rows32[pl.ds(j, runs, stride=SPAN), :] for j in range(SPAN)]
    low8 = low_half((runs, LANES))
    flat_k = jnp.concatenate(
        [
            jnp.where(low8, steps[j], pltpu.roll(steps[j + 1], HEAD_DIM, 1))
            for j in range(0, SPAN, 2)
        ],
        axis=1,
    ).astype(BF16)
    flat_v = jnp.concatenate(
        [
            jnp.where(low8, pltpu.roll(steps[j], HEAD_DIM, 1), steps[j + 1])
            for j in range(0, SPAN, 2)
        ],
        axis=1,
    ).astype(BF16)
    kin_c.wait()
    vin_c.wait()
    kout_c.wait()
    vout_c.wait()
    hidden_k = jax.nn.gelu(dot_t(flat_k, kin[...])).astype(BF16)
    hidden_v = jax.nn.gelu(dot_t(flat_v, vin[...])).astype(BF16)
    sum_k = dot(hidden_k, kout[...]).astype(BF16).astype(F32)
    sum_v = dot(hidden_v, vout[...]).astype(BF16).astype(F32)

    mine = pl.ds(pl.multiple_of(me * runs, runs), runs)
    sums[mine, :] = jnp.concatenate([sum_k, sum_v], axis=1)
    yours = pl.ds(pl.multiple_of((z * inner + lax.rem(y + 1, inner)) * runs, runs), runs)

    def sum_swap(slot):
        return pltpu.make_async_remote_copy(
            src_ref=sums.at[slot, :],
            dst_ref=sums.at[slot, :],
            send_sem=send_s.at[z],
            recv_sem=recv_s.at[z],
            device_id=partner(),
            device_id_type=MESH,
        )

    if inner == 2:
        sum_swap(mine).start()

    def sum_copy(source, target):
        both = inner * runs
        slot = sums.at[pl.ds(pl.multiple_of(source * both, both), both), :]
        return pltpu.make_async_remote_copy(
            src_ref=slot,
            dst_ref=slot,
            send_sem=send_s.at[target],
            recv_sem=recv_s.at[source],
            device_id={"kv": target * inner + y},
            device_id_type=MESH,
        )

    send_at(1)

    qw_c.wait()
    queries = dot(tok[...], qw[...]) * (HEAD_DIM**-0.5 * LOG2E)

    send_at(2)
    low64 = low_half((BLOCK, LANES))
    row_in = lax.broadcasted_iota(jnp.int32, (BLOCK, 1), 0)
    lane = lax.broadcasted_iota(jnp.int32, (1, LANES), 1)
    unit = jnp.where(lane - HEAD_DIM == row_in, 1.0, 0.0)
    for b in range(blocks):
        rows = slice(b * BLOCK, (b + 1) * BLOCK)
        for p in range(pairs):
            two = queries[rows, p * LANES : (p + 1) * LANES]
            at = 2 * p * BLOCK
            stacked[b, at : at + BLOCK] = jnp.where(low64, two, unit).astype(BF16)
            stacked[b, at + BLOCK : at + 2 * BLOCK] = jnp.where(
                low64, pltpu.roll(two, HEAD_DIM, 1), unit
            ).astype(BF16)
    send_at(3)
    def forward(step, carry):
        is_near = jnp.where((step == 1) | (g == 1), 1, 0)
        source = is_near * (z - step) + (1 - is_near) * (step - 2)
        for part in range(PARTS):
            z_copy(source, z, part).wait_recv()

            @pl.when(passes(source))
            def _():
                pass_on(source, part).start()

            if inner == 2:
                y_copy(source, y, part).start()
        return carry

    def first_forward():
        lax.fori_loop(1, jnp.minimum(z, 1) + 1, forward, 0)

    first_forward()


    gw_c.wait()
    gates = jax.nn.sigmoid(dot_t(tok[...], gw[...]))
    half = gates.shape[1] // 2
    gate_s = jnp.where(g == 0, gates[:, :heads], gates[:, heads:half])
    gate_c = jnp.where(g == 0, gates[:, half : half + heads], gates[:, half + heads :])
    send_at(5)
    for b in range(blocks):
        rows = slice(b * BLOCK, (b + 1) * BLOCK)
        for h in range(heads):
            at = slice(h * BLOCK, (h + 1) * BLOCK)
            gate_wide[b, at] = jnp.broadcast_to(gate_c[rows, h : h + 1], (BLOCK, LANES))
            summary_mix[b, at] = jnp.broadcast_to(gate_s[rows, h : h + 1], (BLOCK, LANES))

    def sum_send(target, carry):
        @pl.when((z > 0) & (target > z + 1))
        def _():
            pl.semaphore_wait(ready.at[target], 1)

        sum_copy(z, target).start()
        return carry

    send_at(4)
    if inner == 2:
        sum_swap(yours).wait_recv()
    lax.fori_loop(z + 1, outer, sum_send, 0)

    lax.fori_loop(2, z + 1, forward, 0)

    def sum_wait(source, carry):
        sum_copy(source, z).wait_recv()
        return carry

    lax.fori_loop(0, z, sum_wait, 0)
    sums_kv = sums[...].astype(BF16)
    total_runs = sums_kv.shape[0]
    low_runs = low_half((total_runs, LANES))
    sums_1 = jnp.concatenate([sums_kv, jnp.ones_like(sums_kv)], axis=1)
    run_end = lax.broadcasted_iota(jnp.int32, (total_runs, 1), 0) * SPAN + SPAN - 1
    tall_row = lax.rem(lax.broadcasted_iota(jnp.int32, (heads * BLOCK, 1), 0), BLOCK)
    for b in range(blocks):
        first_row = me * local + b * BLOCK
        barred = jnp.where(run_end <= first_row + lane - HEAD_DIM, 0.0, -1e30).astype(BF16)
        scores = dot_t(stacked[b], jnp.where(low_runs, sums_kv, barred))
        top = jnp.max(scores, axis=1, keepdims=True)
        weights = jnp.exp2(scores - top).astype(BF16)
        o_s = dot(weights, sums_1)
        part = summary_mix[b] * o_s[:, :LANES] / o_s[:, LANES:]
        summary_mix[b] = jnp.where(first_row + tall_row >= SPAN - 1, part, 0.0)

    sel_c.wait()
    ow_c.wait()
    if inner == 2:

        def y_wait(step, carry):
            pltpu.make_async_copy(full(me), full(me), recv_y.at[z - step]).wait()
            return carry

        lax.fori_loop(1 - y, z + 1, y_wait, 0)

    later_key = jnp.where(row_in <= lane - HEAD_DIM, 0.0, -1e30).astype(BF16)
    tall = 2 * LANES
    pieces = [(b, c) for b in range(blocks) for c in range(cols // tall)]
    left, right = {}, {}

    def scores_of(b, c):
        if c == 0:
            score_rows, value_rows = [], []
            for s in range(picks):
                index = sel[0, b, s]
                kv = gathered[jnp.maximum(index, 0)]
                bar = later_key
                if s > 0:
                    bar = jnp.full((BLOCK, LANES), jnp.where(index >= 0, 0.0, -1e30), F32)
                    bar = bar.astype(BF16)
                score_rows.append(jnp.where(low64, kv, bar))
                value_rows.append(kv)
            left[b] = jnp.concatenate(score_rows, axis=0)
            kv = jnp.concatenate(value_rows, axis=0)
            right[b] = jnp.concatenate([kv, jnp.ones_like(kv)], axis=1)
        return dot_t(stacked[b, c * tall : (c + 1) * tall, :], left[b])

    queue = [scores_of(*piece) for piece in pieces[:AHEAD]]
    for i, (b, c) in enumerate(pieces):
        rows = slice(b * BLOCK, (b + 1) * BLOCK)
        at = slice(c * tall, (c + 1) * tall)
        scores = queue.pop(0)
        if i + AHEAD < len(pieces):
            queue.append(scores_of(*pieces[i + AHEAD]))
        top = jnp.max(scores, axis=1, keepdims=True)
        weights = jnp.exp2(scores - top).astype(BF16)
        o_c = dot(weights, right[b])
        mixed = summary_mix[b, at] + gate_wide[b, at] * (o_c[:, :LANES] / o_c[:, LANES:])
        for p in range(tall // LANES):
            even = mixed[2 * p * BLOCK : (2 * p + 1) * BLOCK]
            odd_head = mixed[(2 * p + 1) * BLOCK : (2 * p + 2) * BLOCK]
            here = (c * tall // LANES + p) * LANES
            own_mix[rows, here : here + LANES] = jnp.where(
                low64, pltpu.roll(even, HEAD_DIM, 1), odd_head
            ).astype(BF16)
        if c < cols // tall - 1:
            continue
        mix = pltpu.make_async_remote_copy(
            src_ref=own_mix.at[rows],
            dst_ref=peer_mix.at[rows],
            send_sem=send_m.at[0],
            recv_sem=recv_m.at[0],
            device_id={"tp": 1 - g},
            device_id_type=MESH,
        )
        mix.start()

    own_rows = pl.ds(pl.multiple_of(g * cols, cols), cols)
    peer_rows = pl.ds(pl.multiple_of((1 - g) * cols, cols), cols)
    partial[...] = dot(own_mix[...], ow[own_rows, :])
    all_mixes = pltpu.make_async_remote_copy(
        src_ref=own_mix,
        dst_ref=peer_mix,
        send_sem=send_m.at[0],
        recv_sem=recv_m.at[0],
        device_id={"tp": 1 - g},
        device_id_type=MESH,
    )
    all_mixes.wait_recv()
    out_ref[...] = (partial[...] + dot(peer_mix[...], ow[peer_rows, :])).astype(BF16)
    all_mixes.wait_send()

    def z_done(target, carry):
        pltpu.make_async_copy(full(me), full(me), send_z.at[target]).wait()
        return carry

    last = jnp.where(z == 0, outer, jnp.minimum(z + 2, outer))
    lax.fori_loop(z + 1, last, z_done, 0)

    def pass_done(source, carry):
        pltpu.make_async_copy(full(me), full(me), send_w.at[source]).wait()
        return carry

    lax.fori_loop(1, jnp.where(z < outer - 1, z, 1), pass_done, 0)

    def sum_done(target, carry):
        sum_copy(z, target).wait_send()
        return carry

    lax.fori_loop(z + 1, outer, sum_done, 0)
    if inner == 2:
        sum_swap(mine).wait_send()

        def y_done(step, carry):
            pltpu.make_async_copy(full(me), full(me), send_y.at[z - step]).wait()
            return carry

        lax.fori_loop(y, z + 1, y_done, 0)


def per_device(n_kv, tokens, qw, kw, vw, gw, kin, kout, vin, vout, ow, selection):
    gw, kin, vin = gw.T, kin.T, vin.T
    local, width = tokens.shape
    cols = qw.shape[1]
    inner = 2 if n_kv % 2 == 0 else 1
    outer = n_kv // inner
    blocks = local // BLOCK
    runs = local // SPAN
    tall = cols // HEAD_DIM * BLOCK
    hbm = pl.BlockSpec(memory_space=pltpu.HBM)
    dma = pltpu.SemaphoreType.DMA
    vm = pltpu.VMEM
    operands = [
        pltpu.with_memory_space_constraint(a, pltpu.HBM)
        for a in (selection, tokens, qw, kw, vw, gw, kin, kout, vin, vout, ow)
    ]
    return pl.pallas_call(
        functools.partial(kernel, n_kv, inner),
        out_shape=pltpu.VMEM((local, ow.shape[1]), BF16),
        in_specs=[hbm] * 11,
        out_specs=pl.BlockSpec(memory_space=pltpu.VMEM),
        scratch_shapes=[
            pltpu.SMEM(selection.shape, jnp.int32),
            vm(tokens.shape, BF16),
            vm(qw.shape, BF16),
            vm((width, 2 * LANES), BF16),
            vm(gw.shape, BF16),
            vm(kin.shape, BF16),
            vm(kout.shape, BF16),
            vm(vin.shape, BF16),
            vm(vout.shape, BF16),
            vm(ow.shape, BF16),
            vm((local, LANES), F32),
            vm((n_kv * blocks, BLOCK, LANES), BF16),
            vm((n_kv * runs, LANES), F32),
            vm((blocks, tall, LANES), BF16),
            vm((blocks, tall, LANES), F32),
            vm((blocks, tall, LANES), F32),
            vm((local, cols), BF16),
            vm((local, cols), BF16),
            vm((local, ow.shape[1]), F32),
            dma((CHUNKS + 8,)),
            pltpu.SemaphoreType.REGULAR((outer,)),
            dma((outer,)),
            dma((outer, PARTS)),
            dma((outer,)),
            dma((outer,)),
            dma((outer,)),
            dma((outer,)),
            dma((outer,)),
            dma((1,)),
            dma((1,)),
        ],
        compiler_params=pltpu.CompilerParams(
            collective_id=0, has_side_effects=True, vmem_limit_bytes=GRANT
        ),
        name="attend",
    )(*operands)


def solution(mesh):
    in_specs = (
        P(("dp", "kv"), None),
        P(None, "tp"),
        P(),
        P(),
        P(),
        P(),
        P(),
        P(),
        P(),
        P(None, "tp"),
        P("tp", ("dp", "kv"), None),
    )
    out_specs = P(("dp", "kv"), "tp")
    return jax.shard_map(
        functools.partial(per_device, mesh.shape["kv"]),
        mesh=mesh,
        in_specs=in_specs,
        out_specs=out_specs,
        check_vma=False,
    )
```

```python
import functools

import jax
import jax.numpy as jnp
from jax import lax
from jax.experimental import pallas as pl
from jax.experimental.pallas import tpu as pltpu
from jax.sharding import PartitionSpec as P

HEAD_DIM = 64
BLOCK = 64
SPAN = 32
LANES = 128
MESH = pl.DeviceIdType.MESH
F32 = jnp.float32
BF16 = jnp.bfloat16
CHUNKS = 4
PARTS = 4
SEND_ORDER = ((0, 0, 1), (0, 0, 4))
AHEAD = 8
LOG2E = 1.4426950408889634
GRANT = 40 * 1024 * 1024


def dot(a, b):
    return jnp.dot(a, b, preferred_element_type=F32)


def dot_t(a, b):
    return lax.dot_general(a, b, (((1,), (1,)), ((), ())), preferred_element_type=F32)


def low_half(shape):
    return lax.broadcasted_iota(jnp.int32, shape, len(shape) - 1) < HEAD_DIM


def kernel(
    n_kv,
    inner,
    sel_hbm,
    tok_hbm,
    qw_hbm,
    kw_hbm,
    vw_hbm,
    gw_hbm,
    kin_hbm,
    kout_hbm,
    vin_hbm,
    vout_hbm,
    ow_hbm,
    out_ref,
    sel,
    tok,
    qw,
    kvw,
    gw,
    kin,
    kout,
    vin,
    vout,
    ow,
    rows32,
    gathered,
    sums,
    stacked,
    summary_mix,
    gate_wide,
    own_mix,
    peer_mix,
    partial,
    load_sem,
    ready,
    sent,
    recv_z,
    recv_y,
    send_s,
    recv_s,
    send_m,
    recv_m,
):
    local, width = tok.shape
    runs = local // SPAN
    blocks = local // BLOCK
    cols = qw.shape[1]
    heads = cols // HEAD_DIM
    pairs = cols // LANES
    picks = sel.shape[2]
    outer = n_kv // inner
    me = lax.axis_index("kv")
    g = lax.axis_index("tp")
    z = me // inner
    y = lax.rem(me, inner)

    sums[...] = jnp.zeros_like(sums)
    barrier = pltpu.get_barrier_semaphore()

    def greet(target, carry):
        pl.semaphore_signal(
            barrier, inc=1, device_id={"kv": target * inner + y}, device_id_type=MESH
        )
        return carry

    def partner():
        return {"kv": z * inner + lax.rem(y + 1, inner)}

    lax.fori_loop(z + 1, outer, greet, 0)
    if inner == 2:

        @pl.when(y == 0)
        def _():
            pl.semaphore_signal(barrier, inc=1, device_id=partner(), device_id_type=MESH)

    pl.semaphore_signal(barrier, inc=1, device_id={"tp": 1 - g}, device_id_type=MESH)

    depth = width // CHUNKS
    first = []
    for c in range(CHUNKS):
        part = pl.ds(c * depth, depth)
        trio = [
            pltpu.make_async_copy(tok_hbm.at[:, part], tok.at[:, part], load_sem.at[c]),
            pltpu.make_async_copy(
                kw_hbm.at[part], kvw.at[part, pl.ds(0, LANES)], load_sem.at[c]
            ),
            pltpu.make_async_copy(
                vw_hbm.at[part], kvw.at[part, pl.ds(LANES, LANES)], load_sem.at[c]
            ),
        ]
        for copy in trio:
            copy.start()
        first.append(trio)
    base = CHUNKS
    span_rows = depth * (local + 2 * LANES) // (2 * LANES)
    whole_chunk = kvw.at[pl.ds(0, span_rows)]
    later = [
        pltpu.make_async_copy(src, dst, load_sem.at[base + i])
        for i, (src, dst) in enumerate(
            [
                (kin_hbm, kin),
                (vin_hbm, vin),
                (kout_hbm, kout),
                (vout_hbm, vout),
                (qw_hbm, qw),
                (gw_hbm, gw),
                (sel_hbm, sel),
                (ow_hbm, ow),
            ]
        )
    ]
    kin_c, vin_c, kout_c, vout_c, qw_c, gw_c, sel_c, ow_c = later


    pl.semaphore_wait(barrier, z + y + 1)

    def tell(step, carry):
        pl.semaphore_signal(
            ready.at[z], inc=1, device_id={"kv": (z - step) * inner + y}, device_id_type=MESH
        )
        return carry

    lax.fori_loop(1, z + 1, tell, 0)
    if inner == 2:

        @pl.when(y == 1)
        def _():
            pl.semaphore_signal(ready.at[z], inc=1, device_id=partner(), device_id_type=MESH)

    acc = jnp.zeros((local, 2 * LANES), F32)
    for c in range(CHUNKS):
        pltpu.make_async_copy(whole_chunk, whole_chunk, load_sem.at[c]).wait()
        if c == 0:
            for copy in later[:4]:
                copy.start()
        if c == CHUNKS - 2:
            for copy in later[4:]:
                copy.start()
        part = pl.ds(c * depth, depth)
        acc += dot(tok[:, part], kvw[part, :])
    keys = acc[:, :LANES]
    values = acc[:, LANES:]
    low = low_half((local, LANES))
    paired = jnp.where(
        g == 0,
        jnp.where(low, keys, pltpu.roll(values, HEAD_DIM, 1)),
        jnp.where(low, pltpu.roll(keys, HEAD_DIM, 1), values),
    ).astype(BF16)
    gathered[pl.ds(me * blocks, blocks)] = paired.reshape(blocks, BLOCK, LANES)
    rows32[...] = paired.astype(F32)

    part_blocks = blocks // PARTS

    def full(index):
        return gathered.at[pl.ds(index * blocks, blocks)]

    def slot(index, part):
        return gathered.at[pl.ds(index * blocks + part * part_blocks, part_blocks)]

    def z_copy(source_z, target_z, part):
        return pltpu.make_async_remote_copy(
            src_ref=slot(source_z * inner + y, part),
            dst_ref=slot(source_z * inner + y, part),
            send_sem=sent.at[0],
            recv_sem=recv_z.at[source_z, part],
            device_id={"kv": target_z * inner + y},
            device_id_type=MESH,
        )

    def y_copy(source_z, source_y, part):
        return pltpu.make_async_remote_copy(
            src_ref=slot(source_z * inner + source_y, part),
            dst_ref=slot(source_z * inner + source_y, part),
            send_sem=sent.at[0],
            recv_sem=recv_y.at[source_z],
            device_id={"kv": z * inner + lax.rem(y + 1, inner)},
            device_id_type=MESH,
        )

    def z_send(target, carry):
        pl.semaphore_wait(ready.at[target], 1)
        for part in range(PARTS):
            z_copy(z, target, part).start()
        return carry

    def send_near():
        lax.fori_loop(jnp.minimum(z + 1, outer), jnp.minimum(z + 2, outer), z_send, 0)

    def send_far():
        @pl.when(z == 0)
        def _():
            lax.fori_loop(min(2, outer), outer, z_send, 0)

    def pass_on(source_z, part):
        return pltpu.make_async_remote_copy(
            src_ref=slot(source_z * inner + y, part),
            dst_ref=slot(source_z * inner + y, part),
            send_sem=sent.at[0],
            recv_sem=recv_z.at[source_z, part],
            device_id={"kv": (z + 1) * inner + y},
            device_id_type=MESH,
        )

    def pass_across(source_z, part):
        return pltpu.make_async_remote_copy(
            src_ref=slot(source_z * inner + y, part),
            dst_ref=slot(source_z * inner + y, part),
            send_sem=sent.at[0],
            recv_sem=recv_y.at[source_z],
            device_id={"kv": (z + 1) * inner},
            device_id_type=MESH,
        )

    def crosses():
        return (y == 1) & (g == 0) if inner == 2 else False

    def handed_over(source_z):
        return crosses() & (source_z > 0) & (source_z < z - 1)

    def passes(source_z):
        return (source_z > 0) & (z < outer - 1)

    def send_across():
        if inner == 2:

            @pl.when(y == 0)
            def _():
                pl.semaphore_wait(ready.at[z], 1)
                for part in range(PARTS):
                    y_copy(z, 0, part).start()

    def send_at(point):
        for core, order in enumerate(SEND_ORDER):
            jobs = [job for at, job in zip(order, (send_near, send_across, send_far)) if at == point]
            if jobs:

                @pl.when(g == core)
                def _():
                    for job in jobs:
                        job()

    send_at(0)
    steps = [rows32[pl.ds(j, runs, stride=SPAN), :] for j in range(SPAN)]
    low8 = low_half((runs, LANES))
    flat_k = jnp.concatenate(
        [
            jnp.where(low8, steps[j], pltpu.roll(steps[j + 1], HEAD_DIM, 1))
            for j in range(0, SPAN, 2)
        ],
        axis=1,
    ).astype(BF16)
    flat_v = jnp.concatenate(
        [
            jnp.where(low8, pltpu.roll(steps[j], HEAD_DIM, 1), steps[j + 1])
            for j in range(0, SPAN, 2)
        ],
        axis=1,
    ).astype(BF16)
    kin_c.wait()
    vin_c.wait()
    kout_c.wait()
    vout_c.wait()
    hidden_k = jax.nn.gelu(dot_t(flat_k, kin[...])).astype(BF16)
    hidden_v = jax.nn.gelu(dot_t(flat_v, vin[...])).astype(BF16)
    sum_k = dot(hidden_k, kout[...]).astype(BF16).astype(F32)
    sum_v = dot(hidden_v, vout[...]).astype(BF16).astype(F32)

    mine = pl.ds(pl.multiple_of(me * runs, runs), runs)
    sums[mine, :] = jnp.concatenate([sum_k, sum_v], axis=1)
    yours = pl.ds(pl.multiple_of((z * inner + lax.rem(y + 1, inner)) * runs, runs), runs)

    def sum_swap(slot):
        return pltpu.make_async_remote_copy(
            src_ref=sums.at[slot, :],
            dst_ref=sums.at[slot, :],
            send_sem=send_s.at[z],
            recv_sem=recv_s.at[z],
            device_id=partner(),
            device_id_type=MESH,
        )

    if inner == 2:
        sum_swap(mine).start()

    def sum_copy(source, target):
        both = inner * runs
        slot = sums.at[pl.ds(pl.multiple_of(source * both, both), both), :]
        return pltpu.make_async_remote_copy(
            src_ref=slot,
            dst_ref=slot,
            send_sem=send_s.at[target],
            recv_sem=recv_s.at[source],
            device_id={"kv": target * inner + y},
            device_id_type=MESH,
        )

    send_at(1)

    qw_c.wait()
    queries = dot(tok[...], qw[...]) * (HEAD_DIM**-0.5 * LOG2E)

    send_at(2)
    low64 = low_half((BLOCK, LANES))
    row_in = lax.broadcasted_iota(jnp.int32, (BLOCK, 1), 0)
    lane = lax.broadcasted_iota(jnp.int32, (1, LANES), 1)
    unit = jnp.where(lane - HEAD_DIM == row_in, 1.0, 0.0)
    for b in range(blocks):
        rows = slice(b * BLOCK, (b + 1) * BLOCK)
        for p in range(pairs):
            two = queries[rows, p * LANES : (p + 1) * LANES]
            at = 2 * p * BLOCK
            stacked[b, at : at + BLOCK] = jnp.where(low64, two, unit).astype(BF16)
            stacked[b, at + BLOCK : at + 2 * BLOCK] = jnp.where(
                low64, pltpu.roll(two, HEAD_DIM, 1), unit
            ).astype(BF16)
    send_at(3)
    def forward(step, carry):
        is_near = jnp.where((step == 1) | (g == 1), 1, 0)
        source = is_near * (z - step) + (1 - is_near) * (step - 2)
        for part in range(PARTS):
            z_copy(source, z, part).wait_recv()

            @pl.when(passes(source))
            def _():
                pass_on(source, part).start()
                if inner == 2:

                    @pl.when(crosses())
                    def _():
                        pass_across(source, part).start()

            if inner == 2:

                @pl.when(jnp.logical_not(handed_over(source)))
                def _():
                    y_copy(source, y, part).start()

        return carry

    def first_forward():
        lax.fori_loop(1, jnp.minimum(z, 1) + 1, forward, 0)

    first_forward()


    gw_c.wait()
    gates = jax.nn.sigmoid(dot_t(tok[...], gw[...]))
    half = gates.shape[1] // 2
    gate_s = jnp.where(g == 0, gates[:, :heads], gates[:, heads:half])
    gate_c = jnp.where(g == 0, gates[:, half : half + heads], gates[:, half + heads :])
    send_at(5)
    for b in range(blocks):
        rows = slice(b * BLOCK, (b + 1) * BLOCK)
        for h in range(heads):
            at = slice(h * BLOCK, (h + 1) * BLOCK)
            gate_wide[b, at] = jnp.broadcast_to(gate_c[rows, h : h + 1], (BLOCK, LANES))
            summary_mix[b, at] = jnp.broadcast_to(gate_s[rows, h : h + 1], (BLOCK, LANES))

    def sum_send(target, carry):
        @pl.when((z > 0) & (target > z + 1))
        def _():
            pl.semaphore_wait(ready.at[target], 1)

        sum_copy(z, target).start()
        return carry

    send_at(4)
    if inner == 2:
        sum_swap(yours).wait_recv()
    lax.fori_loop(z + 1, outer, sum_send, 0)

    lax.fori_loop(2, z + 1, forward, 0)

    def sum_wait(source, carry):
        sum_copy(source, z).wait_recv()
        return carry

    lax.fori_loop(0, z, sum_wait, 0)
    sums_kv = sums[...].astype(BF16)
    total_runs = sums_kv.shape[0]
    low_runs = low_half((total_runs, LANES))
    sums_1 = jnp.concatenate([sums_kv, jnp.ones_like(sums_kv)], axis=1)
    run_end = lax.broadcasted_iota(jnp.int32, (total_runs, 1), 0) * SPAN + SPAN - 1
    tall_row = lax.rem(lax.broadcasted_iota(jnp.int32, (heads * BLOCK, 1), 0), BLOCK)
    for b in range(blocks):
        first_row = me * local + b * BLOCK
        barred = jnp.where(run_end <= first_row + lane - HEAD_DIM, 0.0, -1e30).astype(BF16)
        scores = dot_t(stacked[b], jnp.where(low_runs, sums_kv, barred))
        top = jnp.max(scores, axis=1, keepdims=True)
        weights = jnp.exp2(scores - top).astype(BF16)
        o_s = dot(weights, sums_1)
        part = summary_mix[b] * o_s[:, :LANES] / o_s[:, LANES:]
        summary_mix[b] = jnp.where(first_row + tall_row >= SPAN - 1, part, 0.0)

    sel_c.wait()
    ow_c.wait()
    if inner == 2:

        def y_wait(step, carry):
            pltpu.make_async_copy(full(me), full(me), recv_y.at[z - step]).wait()
            return carry

        lax.fori_loop(1 - y, z + 1, y_wait, 0)

    later_key = jnp.where(row_in <= lane - HEAD_DIM, 0.0, -1e30).astype(BF16)
    tall = 2 * LANES
    pieces = [(b, c) for b in range(blocks) for c in range(cols // tall)]
    left, right = {}, {}

    def scores_of(b, c):
        if c == 0:
            score_rows, value_rows = [], []
            for s in range(picks):
                index = sel[0, b, s]
                kv = gathered[jnp.maximum(index, 0)]
                bar = later_key
                if s > 0:
                    bar = jnp.full((BLOCK, LANES), jnp.where(index >= 0, 0.0, -1e30), F32)
                    bar = bar.astype(BF16)
                score_rows.append(jnp.where(low64, kv, bar))
                value_rows.append(kv)
            left[b] = jnp.concatenate(score_rows, axis=0)
            kv = jnp.concatenate(value_rows, axis=0)
            right[b] = jnp.concatenate([kv, jnp.ones_like(kv)], axis=1)
        return dot_t(stacked[b, c * tall : (c + 1) * tall, :], left[b])

    queue = [scores_of(*piece) for piece in pieces[:AHEAD]]
    for i, (b, c) in enumerate(pieces):
        rows = slice(b * BLOCK, (b + 1) * BLOCK)
        at = slice(c * tall, (c + 1) * tall)
        scores = queue.pop(0)
        if i + AHEAD < len(pieces):
            queue.append(scores_of(*pieces[i + AHEAD]))
        top = jnp.max(scores, axis=1, keepdims=True)
        weights = jnp.exp2(scores - top).astype(BF16)
        o_c = dot(weights, right[b])
        mixed = summary_mix[b, at] + gate_wide[b, at] * (o_c[:, :LANES] / o_c[:, LANES:])
        for p in range(tall // LANES):
            even = mixed[2 * p * BLOCK : (2 * p + 1) * BLOCK]
            odd_head = mixed[(2 * p + 1) * BLOCK : (2 * p + 2) * BLOCK]
            here = (c * tall // LANES + p) * LANES
            own_mix[rows, here : here + LANES] = jnp.where(
                low64, pltpu.roll(even, HEAD_DIM, 1), odd_head
            ).astype(BF16)
        if c < cols // tall - 1:
            continue
        mix = pltpu.make_async_remote_copy(
            src_ref=own_mix.at[rows],
            dst_ref=peer_mix.at[rows],
            send_sem=send_m.at[0],
            recv_sem=recv_m.at[2 * b // blocks],
            device_id={"tp": 1 - g},
            device_id_type=MESH,
        )
        mix.start()

    own_rows = pl.ds(pl.multiple_of(g * cols, cols), cols)
    peer_rows = pl.ds(pl.multiple_of((1 - g) * cols, cols), cols)
    partial[...] = dot(own_mix[...], ow[own_rows, :])
    half_rows = local // 2
    for part in range(2):
        rows = slice(part * half_rows, (part + 1) * half_rows)
        theirs = peer_mix.at[rows]
        pltpu.make_async_copy(theirs, theirs, recv_m.at[part]).wait()
        out_ref[rows] = (partial[rows] + dot(peer_mix[rows], ow[peer_rows, :])).astype(BF16)
    pltpu.make_async_copy(own_mix, own_mix, send_m.at[0]).wait()

    def z_done(target, carry):
        pltpu.make_async_copy(full(me), full(me), sent.at[0]).wait()
        return carry

    last = jnp.where(z == 0, outer, jnp.minimum(z + 2, outer))
    lax.fori_loop(z + 1, last, z_done, 0)

    def pass_done(source, carry):
        pltpu.make_async_copy(full(me), full(me), sent.at[0]).wait()
        if inner == 2:

            @pl.when(crosses())
            def _():
                pltpu.make_async_copy(full(me), full(me), sent.at[0]).wait()

        return carry

    lax.fori_loop(1, jnp.where(z < outer - 1, z, 1), pass_done, 0)

    def sum_done(target, carry):
        sum_copy(z, target).wait_send()
        return carry

    lax.fori_loop(z + 1, outer, sum_done, 0)
    if inner == 2:
        sum_swap(mine).wait_send()

        def y_done(step, carry):
            @pl.when(jnp.logical_not(handed_over(z - step)))
            def _():
                pltpu.make_async_copy(full(me), full(me), sent.at[0]).wait()

            return carry

        lax.fori_loop(y, z + 1, y_done, 0)


def per_device(n_kv, tokens, qw, kw, vw, gw, kin, kout, vin, vout, ow, selection):
    gw, kin, vin = gw.T, kin.T, vin.T
    local, width = tokens.shape
    cols = qw.shape[1]
    inner = 2 if n_kv % 2 == 0 else 1
    outer = n_kv // inner
    blocks = local // BLOCK
    runs = local // SPAN
    tall = cols // HEAD_DIM * BLOCK
    hbm = pl.BlockSpec(memory_space=pltpu.HBM)
    dma = pltpu.SemaphoreType.DMA
    vm = pltpu.VMEM
    operands = [
        pltpu.with_memory_space_constraint(a, pltpu.HBM)
        for a in (selection, tokens, qw, kw, vw, gw, kin, kout, vin, vout, ow)
    ]
    return pl.pallas_call(
        functools.partial(kernel, n_kv, inner),
        out_shape=pltpu.VMEM((local, ow.shape[1]), BF16),
        in_specs=[hbm] * 11,
        out_specs=pl.BlockSpec(memory_space=pltpu.VMEM),
        scratch_shapes=[
            pltpu.SMEM(selection.shape, jnp.int32),
            vm(tokens.shape, BF16),
            vm(qw.shape, BF16),
            vm((width, 2 * LANES), BF16),
            vm(gw.shape, BF16),
            vm(kin.shape, BF16),
            vm(kout.shape, BF16),
            vm(vin.shape, BF16),
            vm(vout.shape, BF16),
            vm(ow.shape, BF16),
            vm((local, LANES), F32),
            vm((n_kv * blocks, BLOCK, LANES), BF16),
            vm((n_kv * runs, LANES), F32),
            vm((blocks, tall, LANES), BF16),
            vm((blocks, tall, LANES), F32),
            vm((blocks, tall, LANES), F32),
            vm((local, cols), BF16),
            vm((local, cols), BF16),
            vm((local, ow.shape[1]), F32),
            dma((CHUNKS + 8,)),
            pltpu.SemaphoreType.REGULAR((outer,)),
            dma((1,)),
            dma((outer, PARTS)),
            dma((outer,)),
            dma((outer,)),
            dma((outer,)),
            dma((1,)),
            dma((2,)),
        ],
        compiler_params=pltpu.CompilerParams(
            collective_id=0, has_side_effects=True, vmem_limit_bytes=GRANT
        ),
        name="attend",
    )(*operands)


def solution(mesh):
    in_specs = (
        P(("dp", "kv"), None),
        P(None, "tp"),
        P(),
        P(),
        P(),
        P(),
        P(),
        P(),
        P(),
        P(None, "tp"),
        P("tp", ("dp", "kv"), None),
    )
    out_specs = P(("dp", "kv"), "tp")
    return jax.shard_map(
        functools.partial(per_device, mesh.shape["kv"]),
        mesh=mesh,
        in_specs=in_specs,
        out_specs=out_specs,
        check_vma=False,
    )
```

```python
import functools

import jax
import jax.numpy as jnp
from jax import lax
from jax.experimental import pallas as pl
from jax.experimental.pallas import tpu as pltpu
from jax.sharding import PartitionSpec as P

HEAD_DIM = 64
BLOCK = 64
SPAN = 32
LANES = 128
MESH = pl.DeviceIdType.MESH
F32 = jnp.float32
BF16 = jnp.bfloat16
CUTS = (0, 4, 8, 12, 16)
CHUNKS = len(CUTS) - 1
PARTS = 4
SEND_ORDER = ((0, 0, 1), (0, 0, 4))
AHEAD = 8
LOG2E = 1.4426950408889634
GRANT = 40 * 1024 * 1024


def dot(a, b):
    return jnp.dot(a, b, preferred_element_type=F32)


def dot_t(a, b):
    return lax.dot_general(a, b, (((1,), (1,)), ((), ())), preferred_element_type=F32)


def low_half(shape):
    return lax.broadcasted_iota(jnp.int32, shape, len(shape) - 1) < HEAD_DIM


def kernel(
    n_kv,
    inner,
    sel_hbm,
    tok_hbm,
    qw_hbm,
    kw_hbm,
    vw_hbm,
    gw_hbm,
    kin_hbm,
    kout_hbm,
    vin_hbm,
    vout_hbm,
    ow_hbm,
    out_ref,
    sel,
    tok,
    qw,
    kvw,
    gw,
    kin,
    kout,
    vin,
    vout,
    ow,
    rows32,
    gathered,
    sums,
    stacked,
    summary_mix,
    gate_wide,
    own_mix,
    peer_mix,
    partial,
    load_sem,
    ready,
    sent,
    recv_z,
    recv_y,
    send_s,
    recv_s,
    send_m,
    recv_m,
):
    local, width = tok.shape
    runs = local // SPAN
    blocks = local // BLOCK
    cols = qw.shape[1]
    heads = cols // HEAD_DIM
    pairs = cols // LANES
    picks = sel.shape[2]
    outer = n_kv // inner
    me = lax.axis_index("kv")
    g = lax.axis_index("tp")
    z = me // inner
    y = lax.rem(me, inner)

    sums[...] = jnp.zeros_like(sums)
    barrier = pltpu.get_barrier_semaphore()

    def greet(target, carry):
        pl.semaphore_signal(
            barrier, inc=1, device_id={"kv": target * inner + y}, device_id_type=MESH
        )
        return carry

    def partner():
        return {"kv": z * inner + lax.rem(y + 1, inner)}

    lax.fori_loop(z + 1, outer, greet, 0)
    if inner == 2:

        @pl.when(y == 0)
        def _():
            pl.semaphore_signal(barrier, inc=1, device_id=partner(), device_id_type=MESH)

    pl.semaphore_signal(barrier, inc=1, device_id={"tp": 1 - g}, device_id_type=MESH)

    first = []
    for c in range(CHUNKS):
        part = pl.ds(CUTS[c] * width // 16, (CUTS[c + 1] - CUTS[c]) * width // 16)
        trio = [
            pltpu.make_async_copy(tok_hbm.at[:, part], tok.at[:, part], load_sem.at[c]),
            pltpu.make_async_copy(
                kw_hbm.at[part], kvw.at[part, pl.ds(0, LANES)], load_sem.at[c]
            ),
            pltpu.make_async_copy(
                vw_hbm.at[part], kvw.at[part, pl.ds(LANES, LANES)], load_sem.at[c]
            ),
        ]
        for copy in trio:
            copy.start()
        first.append(trio)
    base = CHUNKS
    later = [
        pltpu.make_async_copy(src, dst, load_sem.at[base + i])
        for i, (src, dst) in enumerate(
            [
                (kin_hbm, kin),
                (vin_hbm, vin),
                (kout_hbm, kout),
                (vout_hbm, vout),
                (qw_hbm, qw),
                (gw_hbm, gw),
                (sel_hbm, sel),
                (ow_hbm, ow),
            ]
        )
    ]
    kin_c, vin_c, kout_c, vout_c, qw_c, gw_c, sel_c, ow_c = later


    pl.semaphore_wait(barrier, z + y + 1)

    def tell(step, carry):
        pl.semaphore_signal(
            ready.at[z], inc=1, device_id={"kv": (z - step) * inner + y}, device_id_type=MESH
        )
        return carry

    lax.fori_loop(1, z + 1, tell, 0)
    if inner == 2:

        @pl.when(y == 1)
        def _():
            pl.semaphore_signal(ready.at[z], inc=1, device_id=partner(), device_id_type=MESH)

    acc = jnp.zeros((local, 2 * LANES), F32)
    for c in range(CHUNKS):
        depth = (CUTS[c + 1] - CUTS[c]) * width // 16
        bulk = kvw.at[pl.ds(0, depth * (local + 2 * LANES) // (2 * LANES))]
        pltpu.make_async_copy(bulk, bulk, load_sem.at[c]).wait()
        if c == 0:
            for copy in later[:4]:
                copy.start()
        if c == CHUNKS - 2:
            for copy in later[4:]:
                copy.start()
        part = pl.ds(CUTS[c] * width // 16, (CUTS[c + 1] - CUTS[c]) * width // 16)
        acc += dot(tok[:, part], kvw[part, :])
    keys = acc[:, :LANES]
    values = acc[:, LANES:]
    low = low_half((local, LANES))
    paired = jnp.where(
        g == 0,
        jnp.where(low, keys, pltpu.roll(values, HEAD_DIM, 1)),
        jnp.where(low, pltpu.roll(keys, HEAD_DIM, 1), values),
    ).astype(BF16)
    gathered[pl.ds(me * blocks, blocks)] = paired.reshape(blocks, BLOCK, LANES)
    rows32[...] = paired.astype(F32)

    part_blocks = blocks // PARTS

    def full(index):
        return gathered.at[pl.ds(index * blocks, blocks)]

    def slot(index, part):
        return gathered.at[pl.ds(index * blocks + part * part_blocks, part_blocks)]

    def z_copy(source_z, target_z, part):
        return pltpu.make_async_remote_copy(
            src_ref=slot(source_z * inner + y, part),
            dst_ref=slot(source_z * inner + y, part),
            send_sem=sent.at[0],
            recv_sem=recv_z.at[source_z, part],
            device_id={"kv": target_z * inner + y},
            device_id_type=MESH,
        )

    def y_copy(source_z, source_y, part):
        return pltpu.make_async_remote_copy(
            src_ref=slot(source_z * inner + source_y, part),
            dst_ref=slot(source_z * inner + source_y, part),
            send_sem=sent.at[0],
            recv_sem=recv_y.at[source_z],
            device_id={"kv": z * inner + lax.rem(y + 1, inner)},
            device_id_type=MESH,
        )

    def z_send(target, carry):
        pl.semaphore_wait(ready.at[target], 1)
        for part in range(PARTS):
            z_copy(z, target, part).start()
        return carry

    def send_near():
        lax.fori_loop(jnp.minimum(z + 1, outer), jnp.minimum(z + 2, outer), z_send, 0)

    def send_far():
        @pl.when(z == 0)
        def _():
            lax.fori_loop(min(2, outer), outer, z_send, 0)

    def pass_on(source_z, part):
        return pltpu.make_async_remote_copy(
            src_ref=slot(source_z * inner + y, part),
            dst_ref=slot(source_z * inner + y, part),
            send_sem=sent.at[0],
            recv_sem=recv_z.at[source_z, part],
            device_id={"kv": (z + 1) * inner + y},
            device_id_type=MESH,
        )

    def pass_across(source_z, part):
        return pltpu.make_async_remote_copy(
            src_ref=slot(source_z * inner + y, part),
            dst_ref=slot(source_z * inner + y, part),
            send_sem=sent.at[0],
            recv_sem=recv_y.at[source_z],
            device_id={"kv": (z + 1) * inner},
            device_id_type=MESH,
        )

    def crosses():
        return (y == 1) & (g == 0) if inner == 2 else False

    def handed_over(source_z):
        return crosses() & (source_z > 0) & (source_z < z - 1)

    def passes(source_z):
        return (source_z > 0) & (z < outer - 1)

    def send_across():
        if inner == 2:

            @pl.when(y == 0)
            def _():
                pl.semaphore_wait(ready.at[z], 1)
                for part in range(PARTS):
                    y_copy(z, 0, part).start()

    def send_at(point):
        for core, order in enumerate(SEND_ORDER):
            jobs = [job for at, job in zip(order, (send_near, send_across, send_far)) if at == point]
            if jobs:

                @pl.when(g == core)
                def _():
                    for job in jobs:
                        job()

    send_at(0)
    steps = [rows32[pl.ds(j, runs, stride=SPAN), :] for j in range(SPAN)]
    low8 = low_half((runs, LANES))
    flat_k = jnp.concatenate(
        [
            jnp.where(low8, steps[j], pltpu.roll(steps[j + 1], HEAD_DIM, 1))
            for j in range(0, SPAN, 2)
        ],
        axis=1,
    ).astype(BF16)
    flat_v = jnp.concatenate(
        [
            jnp.where(low8, pltpu.roll(steps[j], HEAD_DIM, 1), steps[j + 1])
            for j in range(0, SPAN, 2)
        ],
        axis=1,
    ).astype(BF16)
    kin_c.wait()
    vin_c.wait()
    kout_c.wait()
    vout_c.wait()
    hidden_k = jax.nn.gelu(dot_t(flat_k, kin[...])).astype(BF16)
    hidden_v = jax.nn.gelu(dot_t(flat_v, vin[...])).astype(BF16)
    sum_k = dot(hidden_k, kout[...]).astype(BF16).astype(F32)
    sum_v = dot(hidden_v, vout[...]).astype(BF16).astype(F32)

    mine = pl.ds(pl.multiple_of(me * runs, runs), runs)
    sums[mine, :] = jnp.concatenate([sum_k, sum_v], axis=1)
    yours = pl.ds(pl.multiple_of((z * inner + lax.rem(y + 1, inner)) * runs, runs), runs)

    def sum_swap(slot):
        return pltpu.make_async_remote_copy(
            src_ref=sums.at[slot, :],
            dst_ref=sums.at[slot, :],
            send_sem=send_s.at[0],
            recv_sem=recv_s.at[z],
            device_id=partner(),
            device_id_type=MESH,
        )

    if inner == 2:
        sum_swap(mine).start()

    def sum_copy(source, target):
        both = inner * runs
        slot = sums.at[pl.ds(pl.multiple_of(source * both, both), both), :]
        return pltpu.make_async_remote_copy(
            src_ref=slot,
            dst_ref=slot,
            send_sem=send_s.at[0],
            recv_sem=recv_s.at[source],
            device_id={"kv": target * inner + y},
            device_id_type=MESH,
        )

    send_at(1)

    qw_c.wait()
    queries = dot(tok[...], qw[...]) * (HEAD_DIM**-0.5 * LOG2E)

    send_at(2)
    low64 = low_half((BLOCK, LANES))
    row_in = lax.broadcasted_iota(jnp.int32, (BLOCK, 1), 0)
    lane = lax.broadcasted_iota(jnp.int32, (1, LANES), 1)
    unit = jnp.where(lane - HEAD_DIM == row_in, 1.0, 0.0)
    for b in range(blocks):
        rows = slice(b * BLOCK, (b + 1) * BLOCK)
        for p in range(pairs):
            two = queries[rows, p * LANES : (p + 1) * LANES]
            at = 2 * p * BLOCK
            stacked[b, at : at + BLOCK] = jnp.where(low64, two, unit).astype(BF16)
            stacked[b, at + BLOCK : at + 2 * BLOCK] = jnp.where(
                low64, pltpu.roll(two, HEAD_DIM, 1), unit
            ).astype(BF16)
    send_at(3)
    def forward(step, carry):
        is_near = jnp.where((step == 1) | (g == 1), 1, 0)
        source = is_near * (z - step) + (1 - is_near) * (step - 2)
        for part in range(PARTS):
            z_copy(source, z, part).wait_recv()

            @pl.when(passes(source))
            def _():
                pass_on(source, part).start()
                if inner == 2:

                    @pl.when(crosses())
                    def _():
                        pass_across(source, part).start()

            if inner == 2:

                @pl.when(jnp.logical_not(handed_over(source)))
                def _():
                    y_copy(source, y, part).start()

        return carry

    early = jnp.where((g == 0) & (z < outer - 1), 2, 1)

    def first_forward():
        lax.fori_loop(1, jnp.minimum(z, early) + 1, forward, 0)

    first_forward()


    gw_c.wait()
    gates = jax.nn.sigmoid(dot_t(tok[...], gw[...]))
    half = gates.shape[1] // 2
    gate_s = jnp.where(g == 0, gates[:, :heads], gates[:, heads:half])
    gate_c = jnp.where(g == 0, gates[:, half : half + heads], gates[:, half + heads :])
    send_at(5)
    for b in range(blocks):
        rows = slice(b * BLOCK, (b + 1) * BLOCK)
        for h in range(heads):
            at = slice(h * BLOCK, (h + 1) * BLOCK)
            gate_wide[b, at] = jnp.broadcast_to(gate_c[rows, h : h + 1], (BLOCK, LANES))
            summary_mix[b, at] = jnp.broadcast_to(gate_s[rows, h : h + 1], (BLOCK, LANES))

    def sum_send(target, carry):
        @pl.when((z > 0) & (target > z + 1))
        def _():
            pl.semaphore_wait(ready.at[target], 1)

        sum_copy(z, target).start()
        return carry

    send_at(4)
    if inner == 2:
        sum_swap(yours).wait_recv()
    lax.fori_loop(z + 1, outer, sum_send, 0)

    lax.fori_loop(early + 1, z + 1, forward, 0)

    def sum_wait(source, carry):
        sum_copy(source, z).wait_recv()
        return carry

    lax.fori_loop(0, z, sum_wait, 0)
    sums_kv = sums[...].astype(BF16)
    total_runs = sums_kv.shape[0]
    low_runs = low_half((total_runs, LANES))
    sums_1 = jnp.concatenate([sums_kv, jnp.ones_like(sums_kv)], axis=1)
    run_end = lax.broadcasted_iota(jnp.int32, (total_runs, 1), 0) * SPAN + SPAN - 1
    tall_row = lax.rem(lax.broadcasted_iota(jnp.int32, (heads * BLOCK, 1), 0), BLOCK)
    for b in range(blocks):
        first_row = me * local + b * BLOCK
        barred = jnp.where(run_end <= first_row + lane - HEAD_DIM, 0.0, -1e30).astype(BF16)
        scores = dot_t(stacked[b], jnp.where(low_runs, sums_kv, barred))
        top = jnp.max(scores, axis=1, keepdims=True)
        weights = jnp.exp2(scores - top).astype(BF16)
        o_s = dot(weights, sums_1)
        part = summary_mix[b] * o_s[:, :LANES] / o_s[:, LANES:]
        summary_mix[b] = jnp.where(first_row + tall_row >= SPAN - 1, part, 0.0)

    sel_c.wait()
    ow_c.wait()
    if inner == 2:

        def y_wait(step, carry):
            pltpu.make_async_copy(full(me), full(me), recv_y.at[z - step]).wait()
            return carry

        lax.fori_loop(1 - y, z + 1, y_wait, 0)

    later_key = jnp.where(row_in <= lane - HEAD_DIM, 0.0, -1e30).astype(BF16)
    tall = 2 * LANES
    pieces = [(b, c) for b in range(blocks) for c in range(cols // tall)]
    left, right = {}, {}

    def scores_of(b, c):
        if c == 0:
            score_rows, value_rows = [], []
            for s in range(picks):
                index = sel[0, b, s]
                kv = gathered[jnp.maximum(index, 0)]
                bar = later_key
                if s > 0:
                    bar = jnp.full((BLOCK, LANES), jnp.where(index >= 0, 0.0, -1e30), F32)
                    bar = bar.astype(BF16)
                score_rows.append(jnp.where(low64, kv, bar))
                value_rows.append(kv)
            left[b] = jnp.concatenate(score_rows, axis=0)
            kv = jnp.concatenate(value_rows, axis=0)
            right[b] = jnp.concatenate([kv, jnp.ones_like(kv)], axis=1)
        return dot_t(stacked[b, c * tall : (c + 1) * tall, :], left[b])

    queue = [scores_of(*piece) for piece in pieces[:AHEAD]]
    for i, (b, c) in enumerate(pieces):
        rows = slice(b * BLOCK, (b + 1) * BLOCK)
        at = slice(c * tall, (c + 1) * tall)
        scores = queue.pop(0)
        if i + AHEAD < len(pieces):
            queue.append(scores_of(*pieces[i + AHEAD]))
        top = jnp.max(scores, axis=1, keepdims=True)
        weights = jnp.exp2(scores - top).astype(BF16)
        o_c = dot(weights, right[b])
        mixed = summary_mix[b, at] + gate_wide[b, at] * (o_c[:, :LANES] / o_c[:, LANES:])
        for p in range(tall // LANES):
            even = mixed[2 * p * BLOCK : (2 * p + 1) * BLOCK]
            odd_head = mixed[(2 * p + 1) * BLOCK : (2 * p + 2) * BLOCK]
            here = (c * tall // LANES + p) * LANES
            own_mix[rows, here : here + LANES] = jnp.where(
                low64, pltpu.roll(even, HEAD_DIM, 1), odd_head
            ).astype(BF16)
        if c < cols // tall - 1:
            continue
        mix = pltpu.make_async_remote_copy(
            src_ref=own_mix.at[rows],
            dst_ref=peer_mix.at[rows],
            send_sem=send_m.at[0],
            recv_sem=recv_m.at[2 * b // blocks],
            device_id={"tp": 1 - g},
            device_id_type=MESH,
        )
        mix.start()

    own_rows = pl.ds(pl.multiple_of(g * cols, cols), cols)
    peer_rows = pl.ds(pl.multiple_of((1 - g) * cols, cols), cols)
    partial[...] = dot(own_mix[...], ow[own_rows, :])
    half_rows = local // 2
    for part in range(2):
        rows = slice(part * half_rows, (part + 1) * half_rows)
        theirs = peer_mix.at[rows]
        pltpu.make_async_copy(theirs, theirs, recv_m.at[part]).wait()
        out_ref[rows] = (partial[rows] + dot(peer_mix[rows], ow[peer_rows, :])).astype(BF16)
    pltpu.make_async_copy(own_mix, own_mix, send_m.at[0]).wait()

    def z_done(target, carry):
        pltpu.make_async_copy(full(me), full(me), sent.at[0]).wait()
        return carry

    last = jnp.where(z == 0, outer, jnp.minimum(z + 2, outer))
    lax.fori_loop(z + 1, last, z_done, 0)

    def pass_done(source, carry):
        pltpu.make_async_copy(full(me), full(me), sent.at[0]).wait()
        if inner == 2:

            @pl.when(crosses())
            def _():
                pltpu.make_async_copy(full(me), full(me), sent.at[0]).wait()

        return carry

    lax.fori_loop(1, jnp.where(z < outer - 1, z, 1), pass_done, 0)

    def sum_done(target, carry):
        sum_copy(z, target).wait_send()
        return carry

    lax.fori_loop(z + 1, outer, sum_done, 0)
    if inner == 2:
        sum_swap(mine).wait_send()

        def y_done(step, carry):
            @pl.when(jnp.logical_not(handed_over(z - step)))
            def _():
                pltpu.make_async_copy(full(me), full(me), sent.at[0]).wait()

            return carry

        lax.fori_loop(y, z + 1, y_done, 0)


def per_device(n_kv, tokens, qw, kw, vw, gw, kin, kout, vin, vout, ow, selection):
    gw, kin, vin = gw.T, kin.T, vin.T
    local, width = tokens.shape
    cols = qw.shape[1]
    inner = 2 if n_kv % 2 == 0 else 1
    outer = n_kv // inner
    blocks = local // BLOCK
    runs = local // SPAN
    tall = cols // HEAD_DIM * BLOCK
    hbm = pl.BlockSpec(memory_space=pltpu.HBM)
    dma = pltpu.SemaphoreType.DMA
    vm = pltpu.VMEM
    operands = [
        pltpu.with_memory_space_constraint(a, pltpu.HBM)
        for a in (selection, tokens, qw, kw, vw, gw, kin, kout, vin, vout, ow)
    ]
    return pl.pallas_call(
        functools.partial(kernel, n_kv, inner),
        out_shape=pltpu.VMEM((local, ow.shape[1]), BF16),
        in_specs=[hbm] * 11,
        out_specs=pl.BlockSpec(memory_space=pltpu.VMEM),
        scratch_shapes=[
            pltpu.SMEM(selection.shape, jnp.int32),
            vm(tokens.shape, BF16),
            vm(qw.shape, BF16),
            vm((width, 2 * LANES), BF16),
            vm(gw.shape, BF16),
            vm(kin.shape, BF16),
            vm(kout.shape, BF16),
            vm(vin.shape, BF16),
            vm(vout.shape, BF16),
            vm(ow.shape, BF16),
            vm((local, LANES), F32),
            vm((n_kv * blocks, BLOCK, LANES), BF16),
            vm((n_kv * runs, LANES), F32),
            vm((blocks, tall, LANES), BF16),
            vm((blocks, tall, LANES), F32),
            vm((blocks, tall, LANES), F32),
            vm((local, cols), BF16),
            vm((local, cols), BF16),
            vm((local, ow.shape[1]), F32),
            dma((CHUNKS + 8,)),
            pltpu.SemaphoreType.REGULAR((outer,)),
            dma((1,)),
            dma((outer, PARTS)),
            dma((outer,)),
            dma((1,)),
            dma((outer,)),
            dma((1,)),
            dma((2,)),
        ],
        compiler_params=pltpu.CompilerParams(
            collective_id=0, has_side_effects=True, vmem_limit_bytes=GRANT
        ),
        name="attend",
    )(*operands)


def solution(mesh):
    in_specs = (
        P(("dp", "kv"), None),
        P(None, "tp"),
        P(),
        P(),
        P(),
        P(),
        P(),
        P(),
        P(),
        P(None, "tp"),
        P("tp", ("dp", "kv"), None),
    )
    out_specs = P(("dp", "kv"), "tp")
    return jax.shard_map(
        functools.partial(per_device, mesh.shape["kv"]),
        mesh=mesh,
        in_specs=in_specs,
        out_specs=out_specs,
        check_vma=False,
    )
```
